32 devices in a mesh: sp: 8 (over z, x), tp: 4 (over y, core).
Axes of the slice: x: 2, y: 2, z: 4, core: 2. Of those that a mesh axis runs over, the one named last changes fastest.
Arguments:
- tokens: bfloat16 [4096, 2048], P(('sp', 'tp')), may hold values from -6 to 6
- norm_gain: float32 [2048], replicated, may hold values from 0.1 to 1.9
- pool_in_weight: bfloat16 [2048, 1024], P('sp', 'tp'), may hold values from -0.125 to 0.125
- query_weight: bfloat16 [2048, 1024], P('sp', 'tp'), may hold values from -0.125 to 0.125
- forget_weight: bfloat16 [2048, 1024], P('sp', 'tp'), may hold values from -0.125 to 0.125
- input_weight: bfloat16 [2048, 1024], P('sp', 'tp'), may hold values from -0.125 to 0.125
- forget_gap: float32 [1024], P('tp'), may hold values from 0 to 0.02
- decay_shift: float32 [8, 4096], P('tp', 'sp'), may hold values from -0.42 to 0
- out_gain: float32 [128], replicated, may hold values from 0.1 to 1.9
- pool_out_weight: bfloat16 [1024, 2048], P('tp', 'sp'), may hold values from -0.53033009 to 0.53033009
- recur_out_weight: bfloat16 [1024, 2048], P('tp', 'sp'), may hold values from -0.53033009 to 0.53033009
Outputs:
- mixed_out: bfloat16 [4096, 2048], P(('sp', 'tp'))
The draws below stay inside these ranges and needn't reach their ends.
All inputs are finite; a program needn't handle non-finite values.
Results may differ from the reference program's by a relative error of at most 0.014.
Values may be sent and summed in bfloat16 or wider, within the bound.
A program may use at most 64 MiB of HBM per device.

```python
import jax
import jax.numpy as jnp
from jax import lax

D = 2048
GROUPS = 4
GC = 256
POOL = 1024
REC_HEADS = 8
RDIM = 128
REC = 1024
SPAN = 64
TOK_DEV = 512
SEQ = 4096
N_SP = 8
N_TP = 4


def slow_heads(key):
    order = jax.random.permutation(jax.random.fold_in(key, 11), REC_HEADS)
    return order < REC_HEADS // 2


def draw_forget_gap(key, part):
    slow_decay = slow_heads(key)
    unit = jax.random.uniform(jax.random.fold_in(key, 12), (REC_HEADS, RDIM), jnp.float32)
    slow_gap = jnp.exp(jnp.log(0.2) + unit * jnp.log(5.0)) / SEQ
    fast_gap = jnp.exp(jnp.log(0.01) + unit * jnp.log(2.0))
    gap_values = jnp.where(slow_decay[:, None], slow_gap, fast_gap)
    return gap_values.reshape(REC_HEADS * RDIM).astype(jnp.float32)


def draw_decay_shift(key, part):
    slow_decay = slow_heads(key)
    block_count = SEQ // TOK_DEV
    unit = jax.random.uniform(jax.random.fold_in(key, 13), (REC_HEADS, block_count), jnp.float32)
    slow_rate = jnp.exp(jnp.log(0.1) + unit * jnp.log(5.0)) / SEQ
    fast_rate = jnp.exp(jnp.log(0.005) + unit * jnp.log(3.0))
    rates = jnp.where(slow_decay[:, None], slow_rate, fast_rate)
    drawn_result = -jnp.repeat(rates, TOK_DEV, axis=1)
    third = SEQ // 3
    offsets = jax.random.randint(jax.random.fold_in(key, 14), (REC_HEADS, 3), 0, third)
    spots = offsets + jnp.arange(3, dtype=jnp.int32)[None, :] * third
    depth = jax.random.uniform(jax.random.fold_in(key, 15), (REC_HEADS, 3), jnp.float32, 0.22, 0.4)
    places = jnp.arange(SEQ, dtype=jnp.int32)
    match_count = (places[None, None, :] == spots[:, :, None]).astype(jnp.float32) * depth[:, :, None]
    spike_events = jnp.sum(match_count, axis=1) * slow_decay[:, None].astype(jnp.float32)
    return (drawn_result - spike_events).astype(jnp.float32)


def heavy_columns(key, rows, salt):
    chosen = jax.random.randint(jax.random.fold_in(key, 21), (), 0, N_SP)
    block_width = D // N_SP
    column_block = jnp.arange(D, dtype=jnp.int32) // block_width
    factor = jnp.where(column_block == chosen, 4.0, 1.0).astype(jnp.float32)
    scale = (POOL + REC) ** (-0.5)
    drawn = jnp.clip(jax.random.normal(jax.random.fold_in(key, salt), (rows, D), jnp.float32), -6.0, 6.0)
    return (drawn * factor[None, :] * scale).astype(jnp.float32)


def draw_pool_out_weight(key, part):
    return heavy_columns(key, POOL, 22).astype(jnp.bfloat16)


def draw_recur_out_weight(key, part):
    return heavy_columns(key, REC, 23).astype(jnp.bfloat16)


def shard_levels(key, dims, pieces, least, top_value):
    gain, own = 1.0, jax.random.fold_in(key, 6)
    for axis_at, parts in pieces:
        heights = jnp.exp(jax.random.uniform(jax.random.fold_in(own, axis_at), (parts,), jnp.float32, least / len(pieces), top_value / len(pieces)))
        gain = gain * jnp.repeat(heights, dims[axis_at] // parts).reshape([-1 if axis == axis_at else 1 for axis in range(len(dims))])
    return gain


def noise(own_key, shape, scale, bound, cuts=(), kind=jnp.bfloat16):
    level = shard_levels(own_key, shape, cuts, -0.22, 0.18) if cuts else 1.0
    values = jax.random.normal(own_key, shape, jnp.float32) * scale * level
    return jnp.minimum(jnp.maximum(values, -bound), bound).astype(kind)


def setup_inputs(seed: int = 0) -> dict:
    seeds = jax.random.split(jax.random.key(seed), 12)
    return {
        "tokens": noise(seeds[0], (SEQ, D), 1.0, 6.0, ((0, 32),)),
        "norm_gain": jnp.clip(1.0 + 0.18 * jax.random.normal(seeds[1], (D,), jnp.float32), 0.1, 1.9),
        "pool_in_weight": noise(seeds[2], (D, POOL), D ** -0.5, 0.125, ((0, 8), (1, 4))),
        "query_weight": noise(seeds[3], (D, REC), D ** -0.5, 0.125, ((0, 8), (1, 4))),
        "forget_weight": noise(seeds[4], (D, REC), D ** -0.5, 0.125, ((0, 8), (1, 4))),
        "input_weight": noise(seeds[5], (D, REC), D ** -0.5, 0.125, ((0, 8), (1, 4))),
        "forget_gap": draw_forget_gap(jax.random.fold_in(seeds[11], 71), 0),
        "decay_shift": draw_decay_shift(jax.random.fold_in(seeds[11], 71), 0),
        "out_gain": jnp.clip(1.0 + 0.18 * jax.random.normal(seeds[8], (RDIM,), jnp.float32), 0.1, 1.9),
        "pool_out_weight": draw_pool_out_weight(jax.random.fold_in(seeds[11], 71), 0),
        "recur_out_weight": draw_recur_out_weight(jax.random.fold_in(seeds[11], 71), 0),
    }


EPSILON = 1e-06
EXACT_MATMUL = lax.Precision.HIGHEST

def pooling(pooled_in):
    length = pooled_in.shape[0]
    groups = pooled_in.astype(jnp.float32).reshape(length, GROUPS, GC)
    running = jnp.cumsum(groups, axis=0)
    counter = jnp.arange(1, length + 1, dtype=jnp.float32)[:, None]
    means = []
    for index in range(GROUPS):
        width = 2 ** (index + 1)
        current = running[:, index]
        lagged = jnp.pad(current[:length - width], ((width, 0), (0, 0)))
        means.append((current - lagged) / jnp.minimum(counter, jnp.float32(width)))
    mixed = jnp.stack(means, axis=1) - groups
    return mixed.astype(jnp.bfloat16).reshape(length, GROUPS * GC)

def recurrence(query, forget_pre, values, forget_gap, decay_shift, out_gain):
    length = query.shape[0]
    block_count = length // SPAN
    gate_pre = forget_pre.astype(jnp.float32).reshape(length, REC_HEADS, RDIM)
    opened = forget_gap.reshape(REC_HEADS, RDIM) * jax.nn.sigmoid(-gate_pre)
    log_decay = jnp.log1p(-opened) + decay_shift.T[:, :, None]

    def to_blocks(tensor):
        return tensor.reshape(block_count, SPAN, REC_HEADS, RDIM).transpose(0, 2, 1, 3)
    causal = jnp.tril(jnp.ones((SPAN, SPAN), jnp.bool_))

    def block_step(state_matrix, block):
        query_block, decay_block, key_tile_rows, value_tile_rows = block
        inner_block_output = jnp.cumsum(decay_block, axis=1)
        block_decay_total = inner_block_output[:, -1:, :]
        decayed_query = query_block * jnp.exp(inner_block_output)
        scores = jnp.einsum('htk,hsk->hts', decayed_query, key_tile_rows * jnp.exp(-inner_block_output), precision=EXACT_MATMUL)
        scores = jnp.where(causal, scores, 0.0)
        received_output = jnp.einsum('hts,hsv->htv', scores, value_tile_rows, precision=EXACT_MATMUL)
        received_output = received_output + jnp.einsum('dux,dxs->dus', decayed_query, state_matrix, precision=EXACT_MATMUL)
        growth_factor = jnp.einsum('xgb,xgi->xbi', key_tile_rows * jnp.exp(block_decay_total - inner_block_output), value_tile_rows, precision=EXACT_MATMUL)
        new_state = jnp.exp(block_decay_total[:, 0, :])[:, :, None] * state_matrix + growth_factor
        return (new_state, received_output)
    start_state = jnp.zeros((REC_HEADS, RDIM, RDIM), jnp.float32)
    inputs = (to_blocks(query.astype(jnp.float32)), to_blocks(log_decay), to_blocks(opened), to_blocks(values.astype(jnp.float32)))
    _, received_output = lax.scan(block_step, start_state, inputs)
    received_output = received_output.transpose(0, 2, 1, 3).reshape(length, REC_HEADS, RDIM)
    spread = lax.rsqrt(lax.optimization_barrier(jnp.mean(received_output * received_output, axis=-1, keepdims=True)) + EPSILON)
    normed = received_output * spread * out_gain
    return normed.astype(jnp.bfloat16).reshape(length, REC_HEADS * RDIM)

def reference(tokens, norm_gain, pool_in_weight, query_weight, forget_weight, input_weight, forget_gap, decay_shift, out_gain, pool_out_weight, recur_out_weight):
    floats = tokens.astype(jnp.float32)
    scale = lax.rsqrt(lax.optimization_barrier(jnp.mean(floats * floats, axis=-1, keepdims=True)) + EPSILON)
    normed = (floats * scale * norm_gain).astype(jnp.bfloat16)
    pooled_in = jnp.dot(normed, pool_in_weight, preferred_element_type=jnp.float32).astype(jnp.bfloat16)
    query = jnp.dot(normed, query_weight, preferred_element_type=jnp.float32).astype(jnp.bfloat16)
    forget_pre = jnp.dot(normed, forget_weight, preferred_element_type=jnp.float32).astype(jnp.bfloat16)
    values = jnp.dot(normed, input_weight, preferred_element_type=jnp.float32).astype(jnp.bfloat16)
    pool_mixed = pooling(pooled_in)
    recur_mixed = recurrence(query, forget_pre, values, forget_gap, decay_shift, out_gain)
    pool_share = GROUPS * GC // N_TP
    recur_share = REC_HEADS * RDIM // N_TP
    total = jnp.zeros((tokens.shape[0], D), jnp.float32)
    for index in range(N_TP):
        part = jnp.dot(pool_mixed[:, index * pool_share:(index + 1) * pool_share], pool_out_weight[index * pool_share:(index + 1) * pool_share], preferred_element_type=jnp.float32)
        part = part + jnp.dot(recur_mixed[:, index * recur_share:(index + 1) * recur_share], recur_out_weight[index * recur_share:(index + 1) * recur_share], preferred_element_type=jnp.float32)
        part = lax.optimization_barrier(part.astype(jnp.bfloat16))
        total = total + part.astype(jnp.float32)
    return total.astype(jnp.bfloat16)
```

```python
import functools

import jax
import jax.numpy as jnp
from jax import lax
from jax.experimental import pallas as pl
from jax.experimental.pallas import tpu as pltpu
from jax.sharding import PartitionSpec as P

GROUPS = 4
RDIM = 128
SPAN = 64


EPSILON = 1e-06
EXACT_MATMUL = lax.Precision.HIGHEST


def passed_along(block, axis, distance):
    devices = range(lax.axis_size(axis))
    route = [(i - distance, i) for i in devices if i - distance in devices]
    return lax.ppermute(block, axis, route)


def prefix(part, axis, combine, identity):
    place = lax.axis_index(axis)
    gathered = jax.tree.map(lambda a: lax.all_gather(a, axis), part)
    state = jax.tree.map(lambda a, e: jnp.zeros_like(a) + jnp.asarray(e, a.dtype), part, identity)

    def one(hop, state):
        return combine(
            state, jax.tree.map(lambda a: lax.dynamic_index_in_dim(a, hop, 0, False), gathered)
        )

    return lax.fori_loop(0, place, one, state)


def window_sums(padded, levels, reach):
    length = padded.shape[0] - reach
    results = []
    running = padded
    for level in range(levels):
        width = 2**level
        running = running[width:] + running[:-width]
        offset = reach + 1 - 2 * width
        results.append(lax.slice_in_dim(running, offset, offset + length, axis=0))
    return results


def chain(earlier, later):
    return (earlier[0] * later[0], later[0][:, :, None] * earlier[1] + later[1])


def to_blocks(tensor, block_count, head_count):
    return tensor.reshape(block_count, SPAN, head_count, RDIM).transpose(0, 2, 1, 3)


def local(
    tokens,
    norm_gain,
    pool_in_weight,
    query_weight,
    forget_weight,
    input_weight,
    forget_gap,
    decay_shift,
    out_gain,
    pool_out_weight,
    recur_out_weight,
):
    pool_cols = pool_in_weight.shape[1]
    recur_cols = query_weight.shape[1]
    local_in = jnp.concatenate([pool_in_weight, query_weight, forget_weight, input_weight], axis=1)
    whole_in = lax.all_gather(local_in, "sp", axis=0, tiled=True)
    floats = tokens.astype(jnp.float32)
    scale = lax.rsqrt(jnp.mean(floats * floats, axis=-1, keepdims=True) + EPSILON)
    normed = (floats * scale * norm_gain).astype(jnp.bfloat16)
    pool_weight = whole_in[:, :pool_cols]
    recur_weight = whole_in[:, pool_cols:]
    pooled_in = jnp.dot(
        lax.all_gather(normed, "tp", axis=0, tiled=True),
        pool_weight,
        preferred_element_type=jnp.float32,
    ).astype(jnp.bfloat16)
    recur_in = jnp.dot(
        lax.all_gather(normed, "tp", axis=0, tiled=True),
        recur_weight,
        preferred_element_type=jnp.float32,
    ).astype(jnp.bfloat16)
    query = recur_in[:, :recur_cols].astype(jnp.float32)
    forget_pre = recur_in[:, recur_cols : 2 * recur_cols].astype(jnp.float32)
    values = recur_in[:, 2 * recur_cols :].astype(jnp.float32)
    row_count = pooled_in.shape[0]
    head_count = recur_cols // RDIM
    block_count = row_count // SPAN
    gate_pre = forget_pre.reshape(row_count, head_count, RDIM)
    opened = forget_gap.reshape(head_count, RDIM) * jax.nn.sigmoid(-gate_pre)
    log_decay = jnp.log1p(-opened) + decay_shift.T[:, :, None]
    query_blocks = to_blocks(query, block_count, head_count)
    decay_blocks = to_blocks(log_decay, block_count, head_count)
    key_blocks = to_blocks(opened, block_count, head_count)
    value_blocks = to_blocks(values, block_count, head_count)
    causal = jnp.tril(jnp.ones((SPAN, SPAN), jnp.bool_))
    inner_block_output = jnp.cumsum(decay_blocks, axis=2)
    block_decay_total = inner_block_output[:, :, -1, :]
    decayed_query = query_blocks * jnp.exp(inner_block_output)
    scores = jnp.einsum(
        "bhtk,bhsk->bhts",
        decayed_query,
        key_blocks * jnp.exp(-inner_block_output),
        precision=EXACT_MATMUL,
    )
    scores = jnp.where(causal, scores, 0.0)
    received_output = jnp.einsum("bhts,bhsv->bhtv", scores, value_blocks, precision=EXACT_MATMUL)
    growth_factor = jnp.einsum(
        "bhsk,bhsv->bhkv",
        key_blocks * jnp.exp(block_decay_total[:, :, None, :] - inner_block_output),
        value_blocks,
        precision=EXACT_MATMUL,
    )
    fading = jnp.exp(block_decay_total)

    def carry_step(state_matrix, item):
        return (item[0][:, :, None] * state_matrix + item[1], state_matrix)

    empty_state = jnp.zeros((head_count, RDIM, RDIM), jnp.float32)
    local_state, block_starts = lax.scan(carry_step, empty_state, (fading, growth_factor))
    received_output = received_output + jnp.einsum(
        "bhtk,bhkv->bhtv", decayed_query, block_starts, precision=EXACT_MATMUL
    )
    earlier_total = jnp.cumsum(block_decay_total, axis=0) - block_decay_total
    decay_from_start = query_blocks * jnp.exp(inner_block_output + earlier_total[:, :, None, :])
    device_fade = jnp.exp(jnp.sum(block_decay_total, axis=0))
    reach = 2**GROUPS - 1
    rim = pooled_in[row_count - reach :]
    unit_fade = jnp.ones((head_count, RDIM), jnp.float32)
    previous = passed_along(rim, "sp", 1)
    carried_fade, carried_state = prefix(
        (device_fade, local_state), "sp", chain, (unit_fade, empty_state)
    )
    received_output = received_output + jnp.einsum(
        "fuoy,uyi->fuoi", decay_from_start, carried_state, precision=EXACT_MATMUL
    )
    received_output = received_output.transpose(0, 2, 1, 3).reshape(row_count, head_count, RDIM)
    spread = lax.rsqrt(
        jnp.mean(received_output * received_output, axis=-1, keepdims=True) + EPSILON
    )
    recur_mixed = (
        (received_output * spread * out_gain).astype(jnp.bfloat16).reshape(row_count, recur_cols)
    )
    group = lax.axis_index("tp")
    padded = jnp.concatenate([previous, pooled_in], axis=0).astype(jnp.float32)
    results = window_sums(padded, GROUPS, reach)
    window_sum = results[GROUPS - 1]
    for level in range(GROUPS - 1):
        window_sum = jnp.where(group == level, results[level], window_sum)
    width = jnp.left_shift(jnp.int32(2), group)
    position = lax.axis_index("sp") * row_count + jnp.arange(row_count, dtype=jnp.int32)
    divisor = jnp.minimum(position + 1, width).astype(jnp.float32)[:, None]
    pool_mixed = (window_sum / divisor - pooled_in.astype(jnp.float32)).astype(jnp.bfloat16)
    out_pool, out_recur = (
        lax.all_gather(pool_out_weight, "sp", axis=1, tiled=True),
        lax.all_gather(recur_out_weight, "sp", axis=1, tiled=True),
    )
    partial_value = jnp.dot(pool_mixed, out_pool, preferred_element_type=jnp.float32)
    return lax.psum_scatter(
        (
            partial_value + jnp.dot(recur_mixed, out_recur, preferred_element_type=jnp.float32)
        ).astype(jnp.bfloat16),
        "tp",
        scatter_dimension=0,
        tiled=True,
    )


RING = 4
CHUNK = 128
MESH = pl.DeviceIdType.MESH
NT = (((1,), (1,)), ((), ()))
TN = (((0,), (0,)), ((), ()))


def matmul(a, b, dims=(((1,), (0,)), ((), ()))):
    return lax.dot_general(a, b, dims, preferred_element_type=jnp.float32)


def relay(home, slots, sems, place, partner):
    z, x = place // 2, place % 2
    up = lax.rem(z + 1, RING) * 2 + x
    down = lax.rem(z + RING - 1, RING) * 2 + x
    up_other = up + 1 - 2 * x
    send, recv = sems

    def copy(k, block, owner, target):
        return pltpu.make_async_remote_copy(
            src_ref=block,
            dst_ref=slots.at[owner],
            send_sem=send.at[k],
            recv_sem=recv.at[k],
            device_id={"sp": target},
            device_id_type=MESH,
        )

    copies = [
        copy(0, home, place, partner),
        copy(1, home, place, up),
        copy(2, home, place, down),
        copy(3, slots.at[partner], partner, up),
        copy(4, slots.at[partner], partner, down),
        copy(5, slots.at[down], down, up),
        copy(6, slots.at[up_other], up_other, down),
    ]
    far = lax.rem(z + 2, RING) * 2
    arrivals = [partner, down, up, down + 1 - 2 * x, up_other, far + x, far + 1 - x]
    return copies, arrivals


def fused_kernel(
    blocks,
    parts,
    tokens_ref,
    gain_ref,
    win_ref,
    gap_ref,
    shift_ref,
    out_gain_ref,
    wout_ref,
    out_ref,
    normed,
    win,
    wout,
    acc,
    pooled,
    rim,
    state_out,
    state_in,
    fade_out,
    fade_in,
    dq_ref,
    heard_ref,
    mixed,
    part,
    part_in,
    in_send,
    in_recv,
    out_send,
    out_recv,
    tok_send,
    tok_recv,
    rim_sem,
    state_send,
    state_recv,
    fade_send,
    fade_recv,
    part_send,
    part_recv,
    local_sem,
):
    place, seat = lax.axis_index("sp"), lax.axis_index("tp")
    partner = place + 1 - 2 * (place % 2)
    rows, width = tokens_ref.shape
    depth = win_ref.shape[0]
    cols = win_ref.shape[1] // 4
    length = rows * parts
    heads = cols // RDIM

    barrier = pltpu.get_barrier_semaphore()
    for d in range(1, blocks):
        peer = lax.rem(place + d, blocks)
        pl.semaphore_signal(barrier, inc=1, device_id={"sp": peer}, device_id_type=MESH)
    for d in range(1, parts):
        peer = lax.rem(seat + d, parts)
        pl.semaphore_signal(barrier, inc=1, device_id={"tp": peer}, device_id_type=MESH)
    floats = tokens_ref[...].astype(jnp.float32)
    scale = lax.rsqrt(jnp.mean(floats * floats, axis=-1, keepdims=True) + EPSILON)
    normed[seat] = (floats * scale * gain_ref[...]).astype(jnp.bfloat16)
    own = pltpu.make_async_copy(wout_ref, wout.at[place], local_sem)
    own.start()
    pl.semaphore_wait(barrier, blocks + parts - 2)

    wins, win_from = relay(win_ref, win, (in_send, in_recv), place, partner)
    wouts, _ = relay(wout_ref, wout, (out_send, out_recv), place, partner)
    for k in range(3):
        wins[k].start()
    toks = []
    for d in range(1, parts):
        toks.append(
            pltpu.make_async_remote_copy(
                src_ref=normed.at[seat],
                dst_ref=normed.at[seat],
                send_sem=tok_send.at[d - 1],
                recv_sem=tok_recv.at[d - 1],
                device_id={"tp": lax.rem(seat + d, parts)},
                device_id_type=MESH,
            )
        )
        toks[-1].start()

    def accumulate(block, owner, first=False):
        columns = pl.ds(pl.multiple_of(owner * depth, depth), depth)
        left = normed[:, :, columns].reshape(length, depth)

        @pl.loop(0, 4)
        def _(tile):
            at = pl.ds(pl.multiple_of(tile * cols, cols), cols)
            product = matmul(left, block[:, at])
            if first:
                acc[:, at] = product
            else:
                acc[:, at] += product

    wins[0].wait_recv()
    wins[3].start()
    wins[4].start()
    wins[1].wait_recv()
    wins[5].start()
    wins[2].wait_recv()
    for copy in toks:
        copy.wait_recv()
    accumulate(win_ref, place, True)
    wins[4].wait_recv()
    wins[6].start()
    for k in range(3):
        wouts[k].start()
    for k in range(3):
        accumulate(win.at[win_from[k]], win_from[k])
    wins[3].wait_recv()
    accumulate(win.at[win_from[3]], win_from[3])
    accumulate(win.at[win_from[4]], win_from[4])
    wins[5].wait_recv()
    accumulate(win.at[win_from[5]], win_from[5])
    wins[6].wait_recv()
    accumulate(win.at[win_from[6]], win_from[6])

    pooled[...] = acc[:, :cols].astype(jnp.bfloat16)
    rim_rows = rim.shape[0]
    rims = pltpu.make_async_remote_copy(
        src_ref=pooled.at[pl.ds(length - rim_rows, rim_rows)],
        dst_ref=rim,
        send_sem=rim_sem.at[0],
        recv_sem=rim_sem.at[1],
        device_id={"sp": lax.rem(place + 1, blocks)},
        device_id_type=MESH,
    )
    rims.start()
    wouts[0].wait_recv()
    wouts[3].start()
    wouts[4].start()
    wouts[1].wait_recv()
    wouts[5].start()

    row = lax.broadcasted_iota(jnp.int32, (CHUNK, CHUNK), 0)
    col = lax.broadcasted_iota(jnp.int32, (CHUNK, CHUNK), 1)
    causal = col <= row
    lower = causal.astype(jnp.float32)
    for h in range(heads):
        lanes = slice(h * RDIM, (h + 1) * RDIM)
        state = jnp.zeros((RDIM, RDIM), jnp.float32)
        total = jnp.zeros((1, RDIM), jnp.float32)
        for b in range(length // CHUNK):
            at = slice(b * CHUNK, (b + 1) * CHUNK)

            def taken(kind):
                low = kind * cols + h * RDIM
                return acc[at, low : low + RDIM].astype(jnp.bfloat16)

            query = taken(1).astype(jnp.float32)
            gate = taken(2).astype(jnp.float32)
            values = taken(3)
            opened = gap_ref[:, lanes] * jax.nn.sigmoid(-gate)
            decay = jnp.log1p(-opened) + shift_ref[at, h : h + 1]
            inner = lax.dot_general(
                lower,
                decay,
                (((1,), (0,)), ((), ())),
                precision=EXACT_MATMUL,
                preferred_element_type=jnp.float32,
            )
            last = inner[CHUNK - 1 :, :]
            asked = query * jnp.exp(inner)
            keys = (opened * jnp.exp(-inner)).astype(jnp.bfloat16)
            kept = (opened * jnp.exp(last - inner)).astype(jnp.bfloat16)
            asked16 = asked.astype(jnp.bfloat16)
            scores = jnp.where(causal, matmul(asked16, keys, NT), 0.0)
            heard = matmul(scores.astype(jnp.bfloat16), values)
            if b:
                heard += matmul(asked16, state.astype(jnp.bfloat16), NT)
            heard_ref[at, lanes] = heard
            dq_ref[at, lanes] = (asked * jnp.exp(total)).astype(jnp.bfloat16)
            state = jnp.exp(last) * state + matmul(values, kept, TN)
            total = total + last
        state_out[h] = state.astype(jnp.bfloat16)
        fade_out[h] = jnp.broadcast_to(jnp.exp(total), (8, RDIM))

    wouts[4].wait_recv()
    wouts[6].start()
    states = []
    for d in range(1, blocks):
        peer = {"sp": lax.rem(place + d, blocks)}
        for src, dst, send, recv in (
            (fade_out, fade_in, fade_send, fade_recv),
            (state_out, state_in, state_send, state_recv),
        ):
            copy = pltpu.make_async_remote_copy(
                src_ref=src,
                dst_ref=dst.at[place],
                send_sem=send.at[d - 1],
                recv_sem=recv.at[d - 1],
                device_id=peer,
                device_id_type=MESH,
            )
            copy.start()
            states.append(copy)

    rims.wait_recv()
    before = jnp.where(place > 0, rim[...].astype(jnp.float32), 0.0)
    here = pooled[...].astype(jnp.float32)
    running = jnp.concatenate([before, here], axis=0)
    chosen = None
    for level in range(GROUPS):
        running = running + pltpu.roll(running, 2**level, axis=0)
        chosen = running if level == 0 else jnp.where(seat >= level, running, chosen)
    window = jnp.left_shift(jnp.int32(2), seat)
    position = place * length + lax.broadcasted_iota(jnp.int32, (length, 1), 0)
    divisor = jnp.minimum(position + 1, window).astype(jnp.float32)
    mixed[:, :cols] = (chosen[rim_rows:] / divisor - here).astype(jnp.bfloat16)

    for copy in states:
        copy.wait_recv()
    for h in range(heads):
        lanes = slice(h * RDIM, (h + 1) * RDIM)
        carried = jnp.zeros((RDIM, RDIM), jnp.float32)
        for j in range(blocks - 1):
            grown = fade_in[j, h][:1] * carried + state_in[j, h].astype(jnp.float32)
            carried = jnp.where(j < place, grown, carried)
        heard = heard_ref[:, lanes] + matmul(dq_ref[:, lanes], carried.astype(jnp.bfloat16), NT)
        spread = lax.rsqrt(jnp.mean(heard * heard, axis=-1, keepdims=True) + EPSILON)
        low = cols + h * RDIM
        mixed[:, low : low + RDIM] = (heard * spread * out_gain_ref[...]).astype(jnp.bfloat16)

    own.wait()
    for k in (2, 3, 5, 6):
        wouts[k].wait_recv()
    step = wout.shape[2]
    left = mixed[...]
    sums = []
    for j in range(blocks):
        at = pl.ds(j * step, step)
        part[:, :, at] = matmul(left, wout[j]).astype(jnp.bfloat16).reshape(parts, rows, step)
        if j % 2 == 0:
            continue
        at = pl.ds((j - 1) * step, 2 * step)
        for d in range(1, parts):
            peer = lax.rem(seat + d, parts)
            k = (j // 2) * (parts - 1) + d - 1
            copy = pltpu.make_async_remote_copy(
                src_ref=part.at[peer, :, at],
                dst_ref=part_in.at[d - 1, :, at],
                send_sem=part_send.at[k],
                recv_sem=part_recv.at[k],
                device_id={"tp": peer},
                device_id_type=MESH,
            )
            copy.start()
            sums.append(copy)
    for j in range(blocks // 2):
        at = pl.ds(j * 2 * step, 2 * step)
        total = part[seat, :, at].astype(jnp.float32)
        for d in range(parts - 1):
            sums[j * (parts - 1) + d].wait_recv()
            total = total + part_in[d, :, at].astype(jnp.float32)
        out_ref[:, at] = total.astype(jnp.bfloat16)
    for copy in wins + toks + wouts + [rims] + states + sums:
        copy.wait_send()


def fused(
    blocks,
    parts,
    tokens,
    norm_gain,
    pool_in_weight,
    query_weight,
    forget_weight,
    input_weight,
    forget_gap,
    decay_shift,
    out_gain,
    pool_out_weight,
    recur_out_weight,
):
    rows, width = tokens.shape
    length = rows * parts
    depth, cols = pool_in_weight.shape
    heads = cols // RDIM
    step = pool_out_weight.shape[1]
    win = jnp.concatenate([pool_in_weight, query_weight, forget_weight, input_weight], axis=1)
    wout = jnp.concatenate([pool_out_weight, recur_out_weight], axis=0)
    bf16, f32 = jnp.bfloat16, jnp.float32
    peers, seats = blocks - 1, parts - 1
    sem = pltpu.SemaphoreType.DMA
    return pl.pallas_call(
        functools.partial(fused_kernel, blocks, parts),
        out_shape=jax.ShapeDtypeStruct((rows, width), bf16),
        in_specs=[pl.BlockSpec(memory_space=pltpu.VMEM)] * 7,
        out_specs=pl.BlockSpec(memory_space=pltpu.VMEM),
        scratch_shapes=[
            pltpu.VMEM((parts, rows, width), bf16),
            pltpu.VMEM((blocks, depth, 4 * cols), bf16),
            pltpu.VMEM((blocks, 2 * cols, step), bf16),
            pltpu.VMEM((length, 4 * cols), f32),
            pltpu.VMEM((length, cols), bf16),
            pltpu.VMEM((2**GROUPS, cols), bf16),
            pltpu.VMEM((heads, RDIM, RDIM), bf16),
            pltpu.VMEM((blocks, heads, RDIM, RDIM), bf16),
            pltpu.VMEM((heads, 8, RDIM), f32),
            pltpu.VMEM((blocks, heads, 8, RDIM), f32),
            pltpu.VMEM((length, cols), bf16),
            pltpu.VMEM((length, cols), f32),
            pltpu.VMEM((length, 2 * cols), bf16),
            pltpu.VMEM((parts, rows, width), bf16),
            pltpu.VMEM((seats, rows, width), bf16),
            sem((peers,)),
            sem((peers,)),
            sem((peers,)),
            sem((peers,)),
            sem((seats,)),
            sem((seats,)),
            sem((2,)),
            sem((peers,)),
            sem((peers,)),
            sem((peers,)),
            sem((peers,)),
            sem((seats * blocks // 2,)),
            sem((seats * blocks // 2,)),
            sem,
        ],
        compiler_params=pltpu.CompilerParams(
            collective_id=0, has_side_effects=True, vmem_limit_bytes=60000 * 1024
        ),
    )(
        tokens,
        norm_gain.reshape(1, width),
        win,
        forget_gap.reshape(1, cols),
        decay_shift.T,
        out_gain.reshape(1, RDIM),
        wout,
    )


def solution(mesh):
    blocks, parts = mesh.shape["sp"], mesh.shape["tp"]
    body = functools.partial(fused, blocks, parts) if blocks == 2 * RING else local
    in_specs = (
        P(("sp", "tp"), None),
        P(),
        P("sp", "tp"),
        P("sp", "tp"),
        P("sp", "tp"),
        P("sp", "tp"),
        P("tp"),
        P("tp", "sp"),
        P(),
        P("tp", "sp"),
        P("tp", "sp"),
    )
    out_specs = P(("sp", "tp"), None)
    return jax.shard_map(body, mesh=mesh, in_specs=in_specs, out_specs=out_specs, check_vma=False)
```

```python
import functools

import jax
import jax.numpy as jnp
from jax import lax
from jax.experimental import pallas as pl
from jax.experimental.pallas import tpu as pltpu
from jax.sharding import PartitionSpec as P

GROUPS = 4
RDIM = 128
SPAN = 64


EPSILON = 1e-06
EXACT_MATMUL = lax.Precision.HIGHEST


def passed_along(block, axis, distance):
    devices = range(lax.axis_size(axis))
    route = [(i - distance, i) for i in devices if i - distance in devices]
    return lax.ppermute(block, axis, route)


def prefix(part, axis, combine, identity):
    place = lax.axis_index(axis)
    gathered = jax.tree.map(lambda a: lax.all_gather(a, axis), part)
    state = jax.tree.map(lambda a, e: jnp.zeros_like(a) + jnp.asarray(e, a.dtype), part, identity)

    def one(hop, state):
        return combine(
            state, jax.tree.map(lambda a: lax.dynamic_index_in_dim(a, hop, 0, False), gathered)
        )

    return lax.fori_loop(0, place, one, state)


def window_sums(padded, levels, reach):
    length = padded.shape[0] - reach
    results = []
    running = padded
    for level in range(levels):
        width = 2**level
        running = running[width:] + running[:-width]
        offset = reach + 1 - 2 * width
        results.append(lax.slice_in_dim(running, offset, offset + length, axis=0))
    return results


def chain(earlier, later):
    return (earlier[0] * later[0], later[0][:, :, None] * earlier[1] + later[1])


def to_blocks(tensor, block_count, head_count):
    return tensor.reshape(block_count, SPAN, head_count, RDIM).transpose(0, 2, 1, 3)


def local(
    tokens,
    norm_gain,
    pool_in_weight,
    query_weight,
    forget_weight,
    input_weight,
    forget_gap,
    decay_shift,
    out_gain,
    pool_out_weight,
    recur_out_weight,
):
    pool_cols = pool_in_weight.shape[1]
    recur_cols = query_weight.shape[1]
    local_in = jnp.concatenate([pool_in_weight, query_weight, forget_weight, input_weight], axis=1)
    whole_in = lax.all_gather(local_in, "sp", axis=0, tiled=True)
    floats = tokens.astype(jnp.float32)
    scale = lax.rsqrt(jnp.mean(floats * floats, axis=-1, keepdims=True) + EPSILON)
    normed = (floats * scale * norm_gain).astype(jnp.bfloat16)
    pool_weight = whole_in[:, :pool_cols]
    recur_weight = whole_in[:, pool_cols:]
    pooled_in = jnp.dot(
        lax.all_gather(normed, "tp", axis=0, tiled=True),
        pool_weight,
        preferred_element_type=jnp.float32,
    ).astype(jnp.bfloat16)
    recur_in = jnp.dot(
        lax.all_gather(normed, "tp", axis=0, tiled=True),
        recur_weight,
        preferred_element_type=jnp.float32,
    ).astype(jnp.bfloat16)
    query = recur_in[:, :recur_cols].astype(jnp.float32)
    forget_pre = recur_in[:, recur_cols : 2 * recur_cols].astype(jnp.float32)
    values = recur_in[:, 2 * recur_cols :].astype(jnp.float32)
    row_count = pooled_in.shape[0]
    head_count = recur_cols // RDIM
    block_count = row_count // SPAN
    gate_pre = forget_pre.reshape(row_count, head_count, RDIM)
    opened = forget_gap.reshape(head_count, RDIM) * jax.nn.sigmoid(-gate_pre)
    log_decay = jnp.log1p(-opened) + decay_shift.T[:, :, None]
    query_blocks = to_blocks(query, block_count, head_count)
    decay_blocks = to_blocks(log_decay, block_count, head_count)
    key_blocks = to_blocks(opened, block_count, head_count)
    value_blocks = to_blocks(values, block_count, head_count)
    causal = jnp.tril(jnp.ones((SPAN, SPAN), jnp.bool_))
    inner_block_output = jnp.cumsum(decay_blocks, axis=2)
    block_decay_total = inner_block_output[:, :, -1, :]
    decayed_query = query_blocks * jnp.exp(inner_block_output)
    scores = jnp.einsum(
        "bhtk,bhsk->bhts",
        decayed_query,
        key_blocks * jnp.exp(-inner_block_output),
        precision=EXACT_MATMUL,
    )
    scores = jnp.where(causal, scores, 0.0)
    received_output = jnp.einsum("bhts,bhsv->bhtv", scores, value_blocks, precision=EXACT_MATMUL)
    growth_factor = jnp.einsum(
        "bhsk,bhsv->bhkv",
        key_blocks * jnp.exp(block_decay_total[:, :, None, :] - inner_block_output),
        value_blocks,
        precision=EXACT_MATMUL,
    )
    fading = jnp.exp(block_decay_total)

    def carry_step(state_matrix, item):
        return (item[0][:, :, None] * state_matrix + item[1], state_matrix)

    empty_state = jnp.zeros((head_count, RDIM, RDIM), jnp.float32)
    local_state, block_starts = lax.scan(carry_step, empty_state, (fading, growth_factor))
    received_output = received_output + jnp.einsum(
        "bhtk,bhkv->bhtv", decayed_query, block_starts, precision=EXACT_MATMUL
    )
    earlier_total = jnp.cumsum(block_decay_total, axis=0) - block_decay_total
    decay_from_start = query_blocks * jnp.exp(inner_block_output + earlier_total[:, :, None, :])
    device_fade = jnp.exp(jnp.sum(block_decay_total, axis=0))
    reach = 2**GROUPS - 1
    rim = pooled_in[row_count - reach :]
    unit_fade = jnp.ones((head_count, RDIM), jnp.float32)
    previous = passed_along(rim, "sp", 1)
    carried_fade, carried_state = prefix(
        (device_fade, local_state), "sp", chain, (unit_fade, empty_state)
    )
    received_output = received_output + jnp.einsum(
        "fuoy,uyi->fuoi", decay_from_start, carried_state, precision=EXACT_MATMUL
    )
    received_output = received_output.transpose(0, 2, 1, 3).reshape(row_count, head_count, RDIM)
    spread = lax.rsqrt(
        jnp.mean(received_output * received_output, axis=-1, keepdims=True) + EPSILON
    )
    recur_mixed = (
        (received_output * spread * out_gain).astype(jnp.bfloat16).reshape(row_count, recur_cols)
    )
    group = lax.axis_index("tp")
    padded = jnp.concatenate([previous, pooled_in], axis=0).astype(jnp.float32)
    results = window_sums(padded, GROUPS, reach)
    window_sum = results[GROUPS - 1]
    for level in range(GROUPS - 1):
        window_sum = jnp.where(group == level, results[level], window_sum)
    width = jnp.left_shift(jnp.int32(2), group)
    position = lax.axis_index("sp") * row_count + jnp.arange(row_count, dtype=jnp.int32)
    divisor = jnp.minimum(position + 1, width).astype(jnp.float32)[:, None]
    pool_mixed = (window_sum / divisor - pooled_in.astype(jnp.float32)).astype(jnp.bfloat16)
    out_pool, out_recur = (
        lax.all_gather(pool_out_weight, "sp", axis=1, tiled=True),
        lax.all_gather(recur_out_weight, "sp", axis=1, tiled=True),
    )
    partial_value = jnp.dot(pool_mixed, out_pool, preferred_element_type=jnp.float32)
    return lax.psum_scatter(
        (
            partial_value + jnp.dot(recur_mixed, out_recur, preferred_element_type=jnp.float32)
        ).astype(jnp.bfloat16),
        "tp",
        scatter_dimension=0,
        tiled=True,
    )


RING = 4
CHUNK = 128
MESH = pl.DeviceIdType.MESH
NT = (((1,), (1,)), ((), ()))
TN = (((0,), (0,)), ((), ()))


def matmul(a, b, dims=(((1,), (0,)), ((), ()))):
    return lax.dot_general(a, b, dims, preferred_element_type=jnp.float32)


class Relay:
    def __init__(self, home, slots, send, recv, place, inner):
        z, self.x = place // 2, place % 2
        self.home, self.slots, self.send, self.recv = home, slots, send, recv
        self.place, self.inner, self.began = place, inner, []
        self.partner = place + 1 - 2 * self.x
        mate, half = z + 1 - 2 * (z % 2), z // 2
        self.mate = 2 * mate + self.x
        self.across = 2 * lax.rem(RING + RING - 1 - z, RING) + self.x
        self.middle = (z + half) % 2 == 1
        self.line = [mate, 2 - half, 3 - 3 * half]

    def copy(self, k, owner, target, own=False):
        return pltpu.make_async_remote_copy(
            src_ref=self.home if own else self.slots.at[owner],
            dst_ref=self.slots.at[owner],
            send_sem=self.send.at[k],
            recv_sem=self.recv.at[owner],
            device_id={"sp": target},
            device_id_type=MESH,
        )

    def start(self, k, owner, target, own=False, gated=False):
        copy = self.copy(k, owner, target, own)
        self.began.append((copy, gated))
        if gated:
            pl.when(self.middle)(copy.start)
        else:
            copy.start()

    def arrived(self, owner):
        self.copy(0, owner, self.partner).wait_recv()

    def column(self, k):
        return 2 * self.line[k] + self.x

    def across_x(self, k):
        return 2 * self.line[k] + 1 - self.x

    def open(self):
        self.start(0, self.place, self.partner, own=True)
        self.start(1, self.place, self.mate, own=True)
        self.start(2, self.place, self.across, own=True, gated=True)

    def hop(self, k):
        owner = self.column(k)
        self.arrived(owner)
        target = self.mate if k else self.across
        self.start(3 + 2 * k, owner, target, gated=True)
        self.start(4 + 2 * k, owner, self.partner, gated=self.inner and k == 0)

    def inward(self):
        self.arrived(self.partner)
        self.start(9, self.partner, self.mate, gated=True)

    def close(self):
        for copy, gated in self.began:
            if gated:
                pl.when(self.middle)(copy.wait_send)
            else:
                copy.wait_send()


def fused_kernel(
    blocks,
    parts,
    tokens_ref,
    gain_ref,
    win_ref,
    gap_ref,
    shift_ref,
    out_gain_ref,
    wout_ref,
    out_ref,
    normed,
    win,
    wout,
    acc,
    pooled,
    rim,
    state_out,
    state_in,
    fade_out,
    fade_in,
    dq_ref,
    heard_ref,
    mixed,
    part,
    part_in,
    pair,
    in_send,
    in_recv,
    out_send,
    out_recv,
    tok_send,
    tok_recv,
    rim_sem,
    state_send,
    state_recv,
    fade_send,
    fade_recv,
    part_send,
    part_recv,
    local_sem,
):
    place, seat = lax.axis_index("sp"), lax.axis_index("tp")
    partner = place + 1 - 2 * (place % 2)
    rows, width = tokens_ref.shape
    depth = win_ref.shape[0]
    cols = win_ref.shape[1] // 4
    length = rows * parts
    heads = cols // RDIM

    barrier = pltpu.get_barrier_semaphore()
    for d in range(1, blocks):
        peer = lax.rem(place + d, blocks)
        pl.semaphore_signal(barrier, inc=1, device_id={"sp": peer}, device_id_type=MESH)
    for d in range(1, parts):
        peer = lax.rem(seat + d, parts)
        pl.semaphore_signal(barrier, inc=1, device_id={"tp": peer}, device_id_type=MESH)
    floats = tokens_ref[...].astype(jnp.float32)
    scale = lax.rsqrt(jnp.mean(floats * floats, axis=-1, keepdims=True) + EPSILON)
    normed[seat] = (floats * scale * gain_ref[...]).astype(jnp.bfloat16)
    own = pltpu.make_async_copy(wout_ref, wout.at[place], local_sem)
    own.start()
    pl.semaphore_wait(barrier, blocks + parts - 2)

    wins = Relay(win_ref, win, in_send, in_recv, place, False)
    wouts = Relay(wout_ref, wout, out_send, out_recv, place, True)
    wins.open()
    toks = []
    for d in range(1, parts):
        toks.append(
            pltpu.make_async_remote_copy(
                src_ref=normed.at[seat],
                dst_ref=normed.at[seat],
                send_sem=tok_send.at[d - 1],
                recv_sem=tok_recv.at[d - 1],
                device_id={"tp": lax.rem(seat + d, parts)},
                device_id_type=MESH,
            )
        )
        toks[-1].start()

    def accumulate(block, owner, first=False):
        columns = pl.ds(pl.multiple_of(owner * depth, depth), depth)
        left = normed[:, :, columns].reshape(length, depth)

        @pl.loop(0, 4)
        def _(tile):
            at = pl.ds(pl.multiple_of(tile * cols, cols), cols)
            product = matmul(left, block[:, at])
            if first:
                acc[:, at] = product
            else:
                acc[:, at] += product

    wins.hop(0)
    wins.hop(1)
    for copy in toks:
        copy.wait_recv()
    accumulate(win_ref, place, True)
    wins.hop(2)
    wouts.open()
    for k in range(3):
        accumulate(win.at[wins.column(k)], wins.column(k))
    wins.arrived(partner)
    accumulate(win.at[partner], partner)
    for k in range(3):
        owner = wins.across_x(k)
        wins.arrived(owner)
        accumulate(win.at[owner], owner)

    pooled[...] = acc[:, :cols].astype(jnp.bfloat16)
    rim_rows = rim.shape[0]
    rims = pltpu.make_async_remote_copy(
        src_ref=pooled.at[pl.ds(length - rim_rows, rim_rows)],
        dst_ref=rim,
        send_sem=rim_sem.at[0],
        recv_sem=rim_sem.at[1],
        device_id={"sp": lax.rem(place + 1, blocks)},
        device_id_type=MESH,
    )
    rims.start()
    wouts.hop(0)
    wouts.inward()

    row = lax.broadcasted_iota(jnp.int32, (CHUNK, CHUNK), 0)
    col = lax.broadcasted_iota(jnp.int32, (CHUNK, CHUNK), 1)
    causal = col <= row
    lower = causal.astype(jnp.float32)
    for h in range(heads):
        lanes = slice(h * RDIM, (h + 1) * RDIM)
        state = jnp.zeros((RDIM, RDIM), jnp.float32)
        total = jnp.zeros((1, RDIM), jnp.float32)
        for b in range(length // CHUNK):
            at = slice(b * CHUNK, (b + 1) * CHUNK)

            def taken(kind):
                low = kind * cols + h * RDIM
                return acc[at, low : low + RDIM].astype(jnp.bfloat16)

            query = taken(1).astype(jnp.float32)
            gate = taken(2).astype(jnp.float32)
            values = taken(3)
            opened = gap_ref[:, lanes] * jax.nn.sigmoid(-gate)
            decay = jnp.log1p(-opened) + shift_ref[at, h : h + 1]
            inner = lax.dot_general(
                lower,
                decay,
                (((1,), (0,)), ((), ())),
                precision=EXACT_MATMUL,
                preferred_element_type=jnp.float32,
            )
            last = inner[CHUNK - 1 :, :]
            asked = query * jnp.exp(inner)
            keys = (opened * jnp.exp(-inner)).astype(jnp.bfloat16)
            kept = (opened * jnp.exp(last - inner)).astype(jnp.bfloat16)
            asked16 = asked.astype(jnp.bfloat16)
            scores = jnp.where(causal, matmul(asked16, keys, NT), 0.0)
            heard = matmul(scores.astype(jnp.bfloat16), values)
            if b:
                heard += matmul(asked16, state.astype(jnp.bfloat16), NT)
            heard_ref[at, lanes] = heard
            dq_ref[at, lanes] = (asked * jnp.exp(total)).astype(jnp.bfloat16)
            state = jnp.exp(last) * state + matmul(values, kept, TN)
            total = total + last
        state_out[h] = state.astype(jnp.bfloat16)
        fade_out[h] = jnp.broadcast_to(jnp.exp(total), (8, RDIM))
        if h == 0:
            wouts.hop(1)

    wouts.hop(2)
    states = []
    for d in range(1, blocks):
        peer = {"sp": lax.rem(place + d, blocks)}
        for src, dst, send, recv in (
            (fade_out, fade_in, fade_send, fade_recv),
            (state_out, state_in, state_send, state_recv),
        ):
            copy = pltpu.make_async_remote_copy(
                src_ref=src,
                dst_ref=dst.at[place],
                send_sem=send.at[d - 1],
                recv_sem=recv.at[d - 1],
                device_id=peer,
                device_id_type=MESH,
            )
            copy.start()
            states.append(copy)

    rims.wait_recv()
    before = jnp.where(place > 0, rim[...].astype(jnp.float32), 0.0)
    here = pooled[...].astype(jnp.float32)
    running = jnp.concatenate([before, here], axis=0)
    chosen = None
    for level in range(GROUPS):
        running = running + pltpu.roll(running, 2**level, axis=0)
        chosen = running if level == 0 else jnp.where(seat >= level, running, chosen)
    window = jnp.left_shift(jnp.int32(2), seat)
    position = place * length + lax.broadcasted_iota(jnp.int32, (length, 1), 0)
    divisor = jnp.minimum(position + 1, window).astype(jnp.float32)
    mixed[:, :cols] = (chosen[rim_rows:] / divisor - here).astype(jnp.bfloat16)

    for copy in states:
        copy.wait_recv()
    for h in range(heads):
        lanes = slice(h * RDIM, (h + 1) * RDIM)
        carried = jnp.zeros((RDIM, RDIM), jnp.float32)
        for j in range(blocks - 1):
            grown = fade_in[j, h][:1] * carried + state_in[j, h].astype(jnp.float32)
            carried = jnp.where(j < place, grown, carried)
        heard = heard_ref[:, lanes] + matmul(dq_ref[:, lanes], carried.astype(jnp.bfloat16), NT)
        spread = lax.rsqrt(jnp.mean(heard * heard, axis=-1, keepdims=True) + EPSILON)
        low = cols + h * RDIM
        mixed[:, low : low + RDIM] = (heard * spread * out_gain_ref[...]).astype(jnp.bfloat16)

    own.wait()
    for k in range(3):
        wouts.arrived(wouts.across_x(k))
    step = wout.shape[2]
    left = mixed[...]
    other = 2 * (1 - seat // 2) + seat % 2
    near = seat + 1 - 2 * (seat % 2)
    cross = other + 1 - 2 * (seat % 2)
    sums, chunks = [], []

    def send_part(src, lane, target, at):
        copy = pltpu.make_async_remote_copy(
            src_ref=src,
            dst_ref=part_in.at[lane, :, at],
            send_sem=part_send.at[len(sums)],
            recv_sem=part_recv.at[len(sums)],
            device_id={"tp": target},
            device_id_type=MESH,
        )
        copy.start()
        sums.append(copy)
        return copy

    def pass_on(chunk):
        at, relayed = chunk[0], chunk[1]
        relayed.wait_recv()
        both = part[other, :, at].astype(jnp.float32) + part_in[0, :, at].astype(jnp.float32)
        pair[:, at] = both.astype(jnp.bfloat16)
        chunk.append(send_part(pair.at[:, at], 2, other, at))

    for j in range(0, blocks, 2):
        for i in (j, j + 1):
            at = pl.ds(i * step, step)
            part[:, :, at] = matmul(left, wout[i]).astype(jnp.bfloat16).reshape(parts, rows, step)
        at = pl.ds(j * step, 2 * step)
        relayed = send_part(part.at[cross, :, at], 0, near, at)
        chunks.append([at, relayed, send_part(part.at[near, :, at], 1, near, at)])
        if j:
            pass_on(chunks[-2])
    pass_on(chunks[-1])
    for at, _, nearby, far in chunks:
        nearby.wait_recv()
        total = part[seat, :, at].astype(jnp.float32) + part_in[1, :, at].astype(jnp.float32)
        far.wait_recv()
        out_ref[:, at] = (total + part_in[2, :, at].astype(jnp.float32)).astype(jnp.bfloat16)
    wins.close()
    wouts.close()
    for copy in toks + [rims] + states + sums:
        copy.wait_send()


def fused(
    blocks,
    parts,
    tokens,
    norm_gain,
    pool_in_weight,
    query_weight,
    forget_weight,
    input_weight,
    forget_gap,
    decay_shift,
    out_gain,
    pool_out_weight,
    recur_out_weight,
):
    rows, width = tokens.shape
    length = rows * parts
    depth, cols = pool_in_weight.shape
    heads = cols // RDIM
    step = pool_out_weight.shape[1]
    win = jnp.concatenate([pool_in_weight, query_weight, forget_weight, input_weight], axis=1)
    wout = jnp.concatenate([pool_out_weight, recur_out_weight], axis=0)
    bf16, f32 = jnp.bfloat16, jnp.float32
    peers, seats = blocks - 1, parts - 1
    sem = pltpu.SemaphoreType.DMA
    return pl.pallas_call(
        functools.partial(fused_kernel, blocks, parts),
        out_shape=jax.ShapeDtypeStruct((rows, width), bf16),
        in_specs=[pl.BlockSpec(memory_space=pltpu.VMEM)] * 7,
        out_specs=pl.BlockSpec(memory_space=pltpu.VMEM),
        scratch_shapes=[
            pltpu.VMEM((parts, rows, width), bf16),
            pltpu.VMEM((blocks, depth, 4 * cols), bf16),
            pltpu.VMEM((blocks, 2 * cols, step), bf16),
            pltpu.VMEM((length, 4 * cols), f32),
            pltpu.VMEM((length, cols), bf16),
            pltpu.VMEM((2**GROUPS, cols), bf16),
            pltpu.VMEM((heads, RDIM, RDIM), bf16),
            pltpu.VMEM((blocks, heads, RDIM, RDIM), bf16),
            pltpu.VMEM((heads, 8, RDIM), f32),
            pltpu.VMEM((blocks, heads, 8, RDIM), f32),
            pltpu.VMEM((length, cols), bf16),
            pltpu.VMEM((length, cols), f32),
            pltpu.VMEM((length, 2 * cols), bf16),
            pltpu.VMEM((parts, rows, width), bf16),
            pltpu.VMEM((seats, rows, width), bf16),
            pltpu.VMEM((rows, width), bf16),
            sem((10,)),
            sem((blocks,)),
            sem((10,)),
            sem((blocks,)),
            sem((seats,)),
            sem((seats,)),
            sem((2,)),
            sem((peers,)),
            sem((peers,)),
            sem((peers,)),
            sem((peers,)),
            sem((seats * blocks // 2,)),
            sem((seats * blocks // 2,)),
            sem,
        ],
        compiler_params=pltpu.CompilerParams(
            collective_id=0, has_side_effects=True, vmem_limit_bytes=60000 * 1024
        ),
    )(
        tokens,
        norm_gain.reshape(1, width),
        win,
        forget_gap.reshape(1, cols),
        decay_shift.T,
        out_gain.reshape(1, RDIM),
        wout,
    )


def solution(mesh):
    blocks, parts = mesh.shape["sp"], mesh.shape["tp"]
    body = functools.partial(fused, blocks, parts) if (blocks, parts) == (2 * RING, RING) else local
    in_specs = (
        P(("sp", "tp"), None),
        P(),
        P("sp", "tp"),
        P("sp", "tp"),
        P("sp", "tp"),
        P("sp", "tp"),
        P("tp"),
        P("tp", "sp"),
        P(),
        P("tp", "sp"),
        P("tp", "sp"),
    )
    out_specs = P(("sp", "tp"), None)
    return jax.shard_map(body, mesh=mesh, in_specs=in_specs, out_specs=out_specs, check_vma=False)
```

```python
import functools

import jax
import jax.numpy as jnp
from jax import lax
from jax.experimental import pallas as pl
from jax.experimental.pallas import tpu as pltpu
from jax.sharding import PartitionSpec as P

GROUPS = 4
RDIM = 128
SPAN = 64


EPSILON = 1e-06
EXACT_MATMUL = lax.Precision.HIGHEST


def passed_along(block, axis, distance):
    devices = range(lax.axis_size(axis))
    route = [(i - distance, i) for i in devices if i - distance in devices]
    return lax.ppermute(block, axis, route)


def prefix(part, axis, combine, identity):
    place = lax.axis_index(axis)
    gathered = jax.tree.map(lambda a: lax.all_gather(a, axis), part)
    state = jax.tree.map(lambda a, e: jnp.zeros_like(a) + jnp.asarray(e, a.dtype), part, identity)

    def one(hop, state):
        return combine(
            state, jax.tree.map(lambda a: lax.dynamic_index_in_dim(a, hop, 0, False), gathered)
        )

    return lax.fori_loop(0, place, one, state)


def window_sums(padded, levels, reach):
    length = padded.shape[0] - reach
    results = []
    running = padded
    for level in range(levels):
        width = 2**level
        running = running[width:] + running[:-width]
        offset = reach + 1 - 2 * width
        results.append(lax.slice_in_dim(running, offset, offset + length, axis=0))
    return results


def chain(earlier, later):
    return (earlier[0] * later[0], later[0][:, :, None] * earlier[1] + later[1])


def to_blocks(tensor, block_count, head_count):
    return tensor.reshape(block_count, SPAN, head_count, RDIM).transpose(0, 2, 1, 3)


def local(
    tokens,
    norm_gain,
    pool_in_weight,
    query_weight,
    forget_weight,
    input_weight,
    forget_gap,
    decay_shift,
    out_gain,
    pool_out_weight,
    recur_out_weight,
):
    pool_cols = pool_in_weight.shape[1]
    recur_cols = query_weight.shape[1]
    local_in = jnp.concatenate([pool_in_weight, query_weight, forget_weight, input_weight], axis=1)
    whole_in = lax.all_gather(local_in, "sp", axis=0, tiled=True)
    floats = tokens.astype(jnp.float32)
    scale = lax.rsqrt(jnp.mean(floats * floats, axis=-1, keepdims=True) + EPSILON)
    normed = (floats * scale * norm_gain).astype(jnp.bfloat16)
    pool_weight = whole_in[:, :pool_cols]
    recur_weight = whole_in[:, pool_cols:]
    pooled_in = jnp.dot(
        lax.all_gather(normed, "tp", axis=0, tiled=True),
        pool_weight,
        preferred_element_type=jnp.float32,
    ).astype(jnp.bfloat16)
    recur_in = jnp.dot(
        lax.all_gather(normed, "tp", axis=0, tiled=True),
        recur_weight,
        preferred_element_type=jnp.float32,
    ).astype(jnp.bfloat16)
    query = recur_in[:, :recur_cols].astype(jnp.float32)
    forget_pre = recur_in[:, recur_cols : 2 * recur_cols].astype(jnp.float32)
    values = recur_in[:, 2 * recur_cols :].astype(jnp.float32)
    row_count = pooled_in.shape[0]
    head_count = recur_cols // RDIM
    block_count = row_count // SPAN
    gate_pre = forget_pre.reshape(row_count, head_count, RDIM)
    opened = forget_gap.reshape(head_count, RDIM) * jax.nn.sigmoid(-gate_pre)
    log_decay = jnp.log1p(-opened) + decay_shift.T[:, :, None]
    query_blocks = to_blocks(query, block_count, head_count)
    decay_blocks = to_blocks(log_decay, block_count, head_count)
    key_blocks = to_blocks(opened, block_count, head_count)
    value_blocks = to_blocks(values, block_count, head_count)
    causal = jnp.tril(jnp.ones((SPAN, SPAN), jnp.bool_))
    inner_block_output = jnp.cumsum(decay_blocks, axis=2)
    block_decay_total = inner_block_output[:, :, -1, :]
    decayed_query = query_blocks * jnp.exp(inner_block_output)
    scores = jnp.einsum(
        "bhtk,bhsk->bhts",
        decayed_query,
        key_blocks * jnp.exp(-inner_block_output),
        precision=EXACT_MATMUL,
    )
    scores = jnp.where(causal, scores, 0.0)
    received_output = jnp.einsum("bhts,bhsv->bhtv", scores, value_blocks, precision=EXACT_MATMUL)
    growth_factor = jnp.einsum(
        "bhsk,bhsv->bhkv",
        key_blocks * jnp.exp(block_decay_total[:, :, None, :] - inner_block_output),
        value_blocks,
        precision=EXACT_MATMUL,
    )
    fading = jnp.exp(block_decay_total)

    def carry_step(state_matrix, item):
        return (item[0][:, :, None] * state_matrix + item[1], state_matrix)

    empty_state = jnp.zeros((head_count, RDIM, RDIM), jnp.float32)
    local_state, block_starts = lax.scan(carry_step, empty_state, (fading, growth_factor))
    received_output = received_output + jnp.einsum(
        "bhtk,bhkv->bhtv", decayed_query, block_starts, precision=EXACT_MATMUL
    )
    earlier_total = jnp.cumsum(block_decay_total, axis=0) - block_decay_total
    decay_from_start = query_blocks * jnp.exp(inner_block_output + earlier_total[:, :, None, :])
    device_fade = jnp.exp(jnp.sum(block_decay_total, axis=0))
    reach = 2**GROUPS - 1
    rim = pooled_in[row_count - reach :]
    unit_fade = jnp.ones((head_count, RDIM), jnp.float32)
    previous = passed_along(rim, "sp", 1)
    carried_fade, carried_state = prefix(
        (device_fade, local_state), "sp", chain, (unit_fade, empty_state)
    )
    received_output = received_output + jnp.einsum(
        "fuoy,uyi->fuoi", decay_from_start, carried_state, precision=EXACT_MATMUL
    )
    received_output = received_output.transpose(0, 2, 1, 3).reshape(row_count, head_count, RDIM)
    spread = lax.rsqrt(
        jnp.mean(received_output * received_output, axis=-1, keepdims=True) + EPSILON
    )
    recur_mixed = (
        (received_output * spread * out_gain).astype(jnp.bfloat16).reshape(row_count, recur_cols)
    )
    group = lax.axis_index("tp")
    padded = jnp.concatenate([previous, pooled_in], axis=0).astype(jnp.float32)
    results = window_sums(padded, GROUPS, reach)
    window_sum = results[GROUPS - 1]
    for level in range(GROUPS - 1):
        window_sum = jnp.where(group == level, results[level], window_sum)
    width = jnp.left_shift(jnp.int32(2), group)
    position = lax.axis_index("sp") * row_count + jnp.arange(row_count, dtype=jnp.int32)
    divisor = jnp.minimum(position + 1, width).astype(jnp.float32)[:, None]
    pool_mixed = (window_sum / divisor - pooled_in.astype(jnp.float32)).astype(jnp.bfloat16)
    out_pool, out_recur = (
        lax.all_gather(pool_out_weight, "sp", axis=1, tiled=True),
        lax.all_gather(recur_out_weight, "sp", axis=1, tiled=True),
    )
    partial_value = jnp.dot(pool_mixed, out_pool, preferred_element_type=jnp.float32)
    return lax.psum_scatter(
        (
            partial_value + jnp.dot(recur_mixed, out_recur, preferred_element_type=jnp.float32)
        ).astype(jnp.bfloat16),
        "tp",
        scatter_dimension=0,
        tiled=True,
    )


RING = 4
CHUNK = 128
MESH = pl.DeviceIdType.MESH
NT = (((1,), (1,)), ((), ()))
TN = (((0,), (0,)), ((), ()))


def matmul(a, b, dims=(((1,), (0,)), ((), ()))):
    return lax.dot_general(a, b, dims, preferred_element_type=jnp.float32)


class Relay:
    def __init__(self, slots, send, recv, place, inner):
        z, self.x = place // 2, place % 2
        self.slots, self.send, self.recv = slots, send, recv
        self.place, self.inner, self.began = place, inner, []
        self.partner = place + 1 - 2 * self.x
        mate, half = z + 1 - 2 * (z % 2), z // 2
        self.mate = 2 * mate + self.x
        self.across = 2 * lax.rem(RING + RING - 1 - z, RING) + self.x
        self.middle = (z + half) % 2 == 1
        self.end = (z + half) % 2 == 0
        self.line = [mate, 2 - half, 3 - 3 * half]

    def copy(self, k, owner, target):
        return pltpu.make_async_remote_copy(
            src_ref=self.slots.at[owner],
            dst_ref=self.slots.at[owner],
            send_sem=self.send.at[k],
            recv_sem=self.recv.at[owner],
            device_id={"sp": target},
            device_id_type=MESH,
        )

    def start(self, k, owner, target, gate=None):
        copy = self.copy(k, owner, target)
        self.began.append((copy, gate))
        if gate is None:
            copy.start()
        else:
            pl.when(gate)(copy.start)

    def arrived(self, owner):
        self.copy(0, owner, self.partner).wait_recv()

    def column(self, k):
        return 2 * self.line[k] + self.x

    def across_x(self, k):
        return 2 * self.line[k] + 1 - self.x

    def open(self):
        self.start(0, self.place, self.partner)
        self.start(1, self.place, self.mate)
        self.start(2, self.place, self.across, self.middle)

    def hop(self, k):
        owner = self.column(k)
        self.arrived(owner)
        target = self.mate if k else self.across
        self.start(3 + 2 * k, owner, target, self.middle)
        over_x = self.middle if self.inner and k == 0 else self.end if k == 1 else None
        self.start(4 + 2 * k, owner, self.partner, over_x)

    def inward(self):
        self.arrived(self.partner)
        self.start(9, self.partner, self.across, self.middle)
        if self.inner:
            self.start(10, self.partner, self.mate, self.middle)

    def close(self):
        for copy, gate in self.began:
            if gate is None:
                copy.wait_send()
            else:
                pl.when(gate)(copy.wait_send)


def fused_kernel(
    blocks,
    parts,
    tokens_ref,
    gain_ref,
    pool_in_ref,
    query_ref,
    forget_ref,
    input_ref,
    gap_ref,
    shift_ref,
    out_gain_ref,
    pool_out_ref,
    recur_out_ref,
    out_ref,
    normed,
    win,
    wout,
    acc,
    pooled,
    rim,
    state_out,
    state_near,
    state_pair,
    state_in,
    fade_out,
    fade_near,
    fade_pair,
    fade_in,
    dq_ref,
    heard_ref,
    mixed,
    part,
    part_in,
    pair,
    in_send,
    in_recv,
    out_send,
    out_recv,
    tok_send,
    tok_recv,
    rim_sem,
    state_send,
    state_recv,
    fade_send,
    fade_recv,
    part_send,
    part_recv,
    local_sem,
):
    place, seat = lax.axis_index("sp"), lax.axis_index("tp")
    partner = place + 1 - 2 * (place % 2)
    rows, width = tokens_ref.shape
    depth, cols = pool_in_ref.shape
    z, x = place // 2, place % 2
    length = rows * parts
    heads = cols // RDIM

    staged_in, staged_out = [], []
    for i, ref in enumerate((pool_in_ref, query_ref, forget_ref, input_ref)):
        target = win.at[place, :, pl.ds(i * cols, cols)]
        staged_in.append(pltpu.make_async_copy(ref, target, local_sem.at[i]))
        staged_in[-1].start()
    for i, ref in enumerate((pool_out_ref, recur_out_ref)):
        target = wout.at[place, pl.ds(i * cols, cols)]
        staged_out.append(pltpu.make_async_copy(ref, target, local_sem.at[4 + i]))
        staged_out[-1].start()
    barrier = pltpu.get_barrier_semaphore()
    for d in range(1, blocks):
        peer = lax.rem(place + d, blocks)
        pl.semaphore_signal(barrier, inc=1, device_id={"sp": peer}, device_id_type=MESH)
    for d in range(1, parts):
        peer = lax.rem(seat + d, parts)
        pl.semaphore_signal(barrier, inc=1, device_id={"tp": peer}, device_id_type=MESH)
    floats = tokens_ref[...].astype(jnp.float32)
    scale = lax.rsqrt(jnp.mean(floats * floats, axis=-1, keepdims=True) + EPSILON)
    normed[seat] = (floats * scale * gain_ref[...]).astype(jnp.bfloat16)
    pl.semaphore_wait(barrier, blocks + parts - 2)

    for copy in staged_in:
        copy.wait()
    wins = Relay(win, in_send, in_recv, place, False)
    wouts = Relay(wout, out_send, out_recv, place, True)
    wins.open()
    toks = []
    for d in range(1, parts):
        toks.append(
            pltpu.make_async_remote_copy(
                src_ref=normed.at[seat],
                dst_ref=normed.at[seat],
                send_sem=tok_send.at[d - 1],
                recv_sem=tok_recv.at[d - 1],
                device_id={"tp": lax.rem(seat + d, parts)},
                device_id_type=MESH,
            )
        )
        toks[-1].start()

    def accumulate(block, owner, first=False):
        columns = pl.ds(pl.multiple_of(owner * depth, depth), depth)
        left = normed[:, :, columns].reshape(length, depth)

        @pl.loop(0, 4)
        def _(tile):
            at = pl.ds(pl.multiple_of(tile * cols, cols), cols)
            product = matmul(left, block[:, at])
            if first:
                acc[:, at] = product
            else:
                acc[:, at] += product

    wins.hop(0)
    wins.inward()
    wins.hop(1)
    for copy in toks:
        copy.wait_recv()
    accumulate(win.at[place], place, True)
    wins.hop(2)
    for copy in staged_out:
        copy.wait()
    wouts.open()
    for k in range(3):
        accumulate(win.at[wins.column(k)], wins.column(k))
    accumulate(win.at[partner], partner)
    for k in range(3):
        owner = wins.across_x(k)
        wins.arrived(owner)
        accumulate(win.at[owner], owner)

    pooled[...] = acc[:, :cols].astype(jnp.bfloat16)
    rim_rows = rim.shape[0]
    rims = pltpu.make_async_remote_copy(
        src_ref=pooled.at[pl.ds(length - rim_rows, rim_rows)],
        dst_ref=rim,
        send_sem=rim_sem.at[0],
        recv_sem=rim_sem.at[1],
        device_id={"sp": lax.rem(place + 1, blocks)},
        device_id_type=MESH,
    )
    rims.start()
    wouts.hop(0)
    wouts.inward()

    row = lax.broadcasted_iota(jnp.int32, (CHUNK, CHUNK), 0)
    col = lax.broadcasted_iota(jnp.int32, (CHUNK, CHUNK), 1)
    causal = col <= row
    lower = causal.astype(jnp.float32)
    for h in range(heads):
        lanes = slice(h * RDIM, (h + 1) * RDIM)
        state = jnp.zeros((RDIM, RDIM), jnp.float32)
        total = jnp.zeros((1, RDIM), jnp.float32)
        for b in range(length // CHUNK):
            at = slice(b * CHUNK, (b + 1) * CHUNK)

            def taken(kind):
                low = kind * cols + h * RDIM
                return acc[at, low : low + RDIM].astype(jnp.bfloat16)

            query = taken(1).astype(jnp.float32)
            gate = taken(2).astype(jnp.float32)
            values = taken(3)
            opened = gap_ref[:, lanes] * jax.nn.sigmoid(-gate)
            decay = jnp.log1p(-opened) + jnp.broadcast_to(shift_ref[h : h + 1, at], (RDIM, CHUNK)).T
            inner = lax.dot_general(
                lower,
                decay,
                (((1,), (0,)), ((), ())),
                precision=EXACT_MATMUL,
                preferred_element_type=jnp.float32,
            )
            last = inner[CHUNK - 1 :, :]
            asked = query * jnp.exp(inner)
            keys = (opened * jnp.exp(-inner)).astype(jnp.bfloat16)
            kept = (opened * jnp.exp(last - inner)).astype(jnp.bfloat16)
            asked16 = asked.astype(jnp.bfloat16)
            scores = jnp.where(causal, matmul(asked16, keys, NT), 0.0)
            heard = matmul(scores.astype(jnp.bfloat16), values)
            if b:
                heard += matmul(asked16, state.astype(jnp.bfloat16), NT)
            heard_ref[at, lanes] = heard
            dq_ref[at, lanes] = (asked * jnp.exp(total)).astype(jnp.bfloat16)
            state = jnp.exp(last) * state + matmul(values, kept, TN)
            total = total + last
        state_out[h] = state.astype(jnp.bfloat16)
        fade_out[h] = jnp.broadcast_to(jnp.exp(total), (8, RDIM))

    kinds = (
        (fade_out, fade_near, fade_pair, fade_in, fade_send, fade_recv),
        (state_out, state_near, state_pair, state_in, state_send, state_recv),
    )
    states, later = [], []
    for own, near_ref, _, _, send, recv in kinds:
        copy = pltpu.make_async_remote_copy(
            src_ref=own,
            dst_ref=near_ref,
            send_sem=send.at[0],
            recv_sem=recv.at[0],
            device_id={"sp": partner},
            device_id_type=MESH,
        )
        copy.start()
        states.append(copy)
    wouts.hop(1)
    for copy in states:
        copy.wait_recv()
    for h in range(heads):
        fades = fade_out[h], fade_near[h]
        ours, theirs = state_out[h].astype(jnp.float32), state_near[h].astype(jnp.float32)
        first = jnp.where(x == 0, ours, theirs)
        second = jnp.where(x == 0, theirs, ours)
        fade_pair[h] = fades[0] * fades[1]
        fade = jnp.where(x == 0, fades[1], fades[0])[:1]
        state_pair[h] = (fade * first + second).astype(jnp.bfloat16)
    for d in range(1, RING):
        for _, _, pair_ref, dst, send, recv in kinds:
            copy = pltpu.make_async_remote_copy(
                src_ref=pair_ref,
                dst_ref=dst.at[z],
                send_sem=send.at[d],
                recv_sem=recv.at[d],
                device_id={"sp": lax.rem(place + 2 * d, blocks)},
                device_id_type=MESH,
            )
            pl.when(z + d < RING)(copy.start)
            later.append((d, copy))
    wouts.hop(2)

    rims.wait_recv()
    before = jnp.where(place > 0, rim[...].astype(jnp.float32), 0.0)
    here = pooled[...].astype(jnp.float32)
    running = jnp.concatenate([before, here], axis=0)
    chosen = None
    for level in range(GROUPS):
        running = running + pltpu.roll(running, 2**level, axis=0)
        chosen = running if level == 0 else jnp.where(seat >= level, running, chosen)
    window = jnp.left_shift(jnp.int32(2), seat)
    position = place * length + lax.broadcasted_iota(jnp.int32, (length, 1), 0)
    divisor = jnp.minimum(position + 1, window).astype(jnp.float32)
    mixed[:, :cols] = (chosen[rim_rows:] / divisor - here).astype(jnp.bfloat16)

    for d, copy in later:
        pl.when(z >= d)(copy.wait_recv)
    for h in range(heads):
        lanes = slice(h * RDIM, (h + 1) * RDIM)
        carried = jnp.zeros((RDIM, RDIM), jnp.float32)
        for j in range(RING - 1):
            grown = fade_in[j, h][:1] * carried + state_in[j, h].astype(jnp.float32)
            carried = jnp.where(j < z, grown, carried)
        grown = fade_near[h][:1] * carried + state_near[h].astype(jnp.float32)
        carried = jnp.where(x == 1, grown, carried)
        heard = heard_ref[:, lanes] + matmul(dq_ref[:, lanes], carried.astype(jnp.bfloat16), NT)
        spread = lax.rsqrt(jnp.mean(heard * heard, axis=-1, keepdims=True) + EPSILON)
        low = cols + h * RDIM
        mixed[:, low : low + RDIM] = (heard * spread * out_gain_ref[...]).astype(jnp.bfloat16)

    step = wout.shape[2]
    left = mixed[...]
    other = 2 * (1 - seat // 2) + seat % 2
    near = seat + 1 - 2 * (seat % 2)
    cross = other + 1 - 2 * (seat % 2)
    sums, chunks = [], []

    def send_part(src, lane, target, at):
        copy = pltpu.make_async_remote_copy(
            src_ref=src,
            dst_ref=part_in.at[lane, :, at],
            send_sem=part_send.at[len(sums)],
            recv_sem=part_recv.at[len(sums)],
            device_id={"tp": target},
            device_id_type=MESH,
        )
        copy.start()
        sums.append(copy)
        return copy

    def pass_on(chunk):
        at, relayed = chunk[0], chunk[1]
        relayed.wait_recv()
        both = part[other, :, at].astype(jnp.float32) + part_in[0, :, at].astype(jnp.float32)
        pair[:, at] = both.astype(jnp.bfloat16)
        chunk.append(send_part(pair.at[:, at], 2, other, at))

    for j in range(RING):
        if j:
            wouts.arrived(wouts.across_x(j - 1))
        base = 2 * (wouts.line[j - 1] if j else z)
        for i in (base, base + 1):
            at = pl.ds(pl.multiple_of(i * step, step), step)
            part[:, :, at] = matmul(left, wout[i]).astype(jnp.bfloat16).reshape(parts, rows, step)
        at = pl.ds(pl.multiple_of(base * step, 2 * step), 2 * step)
        relayed = send_part(part.at[cross, :, at], 0, near, at)
        chunks.append([at, relayed, send_part(part.at[near, :, at], 1, near, at)])
        if j:
            pass_on(chunks[-2])
    pass_on(chunks[-1])
    for at, _, nearby, far in chunks:
        nearby.wait_recv()
        total = part[seat, :, at].astype(jnp.float32) + part_in[1, :, at].astype(jnp.float32)
        far.wait_recv()
        out_ref[:, at] = (total + part_in[2, :, at].astype(jnp.float32)).astype(jnp.bfloat16)
    wins.close()
    wouts.close()
    for copy in toks + [rims] + states + sums:
        copy.wait_send()
    for d, copy in later:
        pl.when(z + d < RING)(copy.wait_send)


def fused(
    blocks,
    parts,
    tokens,
    norm_gain,
    pool_in_weight,
    query_weight,
    forget_weight,
    input_weight,
    forget_gap,
    decay_shift,
    out_gain,
    pool_out_weight,
    recur_out_weight,
):
    rows, width = tokens.shape
    length = rows * parts
    depth, cols = pool_in_weight.shape
    heads = cols // RDIM
    step = pool_out_weight.shape[1]
    bf16, f32 = jnp.bfloat16, jnp.float32
    seats = parts - 1
    vmem, whole = pl.BlockSpec(memory_space=pltpu.VMEM), pl.BlockSpec(memory_space=pl.ANY)
    sem = pltpu.SemaphoreType.DMA
    return pl.pallas_call(
        functools.partial(fused_kernel, blocks, parts),
        out_shape=jax.ShapeDtypeStruct((rows, width), bf16),
        in_specs=[vmem] * 2 + [whole] * 4 + [vmem] * 3 + [whole] * 2,
        out_specs=pl.BlockSpec(memory_space=pltpu.VMEM),
        scratch_shapes=[
            pltpu.VMEM((parts, rows, width), bf16),
            pltpu.VMEM((blocks, depth, 4 * cols), bf16),
            pltpu.VMEM((blocks, 2 * cols, step), bf16),
            pltpu.VMEM((length, 4 * cols), f32),
            pltpu.VMEM((length, cols), bf16),
            pltpu.VMEM((2**GROUPS, cols), bf16),
            *[pltpu.VMEM((heads, RDIM, RDIM), bf16)] * 3,
            pltpu.VMEM((RING, heads, RDIM, RDIM), bf16),
            *[pltpu.VMEM((heads, 8, RDIM), f32)] * 3,
            pltpu.VMEM((RING, heads, 8, RDIM), f32),
            pltpu.VMEM((length, cols), bf16),
            pltpu.VMEM((length, cols), f32),
            pltpu.VMEM((length, 2 * cols), bf16),
            pltpu.VMEM((parts, rows, width), bf16),
            pltpu.VMEM((seats, rows, width), bf16),
            pltpu.VMEM((rows, width), bf16),
            sem((11,)),
            sem((blocks,)),
            sem((11,)),
            sem((blocks,)),
            sem((seats,)),
            sem((seats,)),
            sem((2,)),
            sem((RING,)),
            sem((RING,)),
            sem((RING,)),
            sem((RING,)),
            sem((seats * blocks // 2,)),
            sem((seats * blocks // 2,)),
            sem((6,)),
        ],
        compiler_params=pltpu.CompilerParams(
            collective_id=0, has_side_effects=True, vmem_limit_bytes=60000 * 1024
        ),
    )(
        tokens,
        norm_gain.reshape(1, width),
        pool_in_weight,
        query_weight,
        forget_weight,
        input_weight,
        forget_gap.reshape(1, cols),
        decay_shift,
        out_gain.reshape(1, RDIM),
        pool_out_weight,
        recur_out_weight,
    )


def solution(mesh):
    blocks, parts = mesh.shape["sp"], mesh.shape["tp"]
    body = functools.partial(fused, blocks, parts) if (blocks, parts) == (2 * RING, RING) else local
    in_specs = (
        P(("sp", "tp"), None),
        P(),
        P("sp", "tp"),
        P("sp", "tp"),
        P("sp", "tp"),
        P("sp", "tp"),
        P("tp"),
        P("tp", "sp"),
        P(),
        P("tp", "sp"),
        P("tp", "sp"),
    )
    out_specs = P(("sp", "tp"), None)
    return jax.shard_map(body, mesh=mesh, in_specs=in_specs, out_specs=out_specs, check_vma=False)
```

```python
import functools

import jax
import jax.numpy as jnp
from jax import lax
from jax.experimental import pallas as pl
from jax.experimental.pallas import tpu as pltpu
from jax.sharding import PartitionSpec as P

GROUPS = 4
RDIM = 128
SPAN = 64


EPSILON = 1e-06
EXACT_MATMUL = lax.Precision.HIGHEST


def passed_along(block, axis, distance):
    devices = range(lax.axis_size(axis))
    route = [(i - distance, i) for i in devices if i - distance in devices]
    return lax.ppermute(block, axis, route)


def prefix(part, axis, combine, identity):
    place = lax.axis_index(axis)
    gathered = jax.tree.map(lambda a: lax.all_gather(a, axis), part)
    state = jax.tree.map(lambda a, e: jnp.zeros_like(a) + jnp.asarray(e, a.dtype), part, identity)

    def one(hop, state):
        return combine(
            state, jax.tree.map(lambda a: lax.dynamic_index_in_dim(a, hop, 0, False), gathered)
        )

    return lax.fori_loop(0, place, one, state)


def window_sums(padded, levels, reach):
    length = padded.shape[0] - reach
    results = []
    running = padded
    for level in range(levels):
        width = 2**level
        running = running[width:] + running[:-width]
        offset = reach + 1 - 2 * width
        results.append(lax.slice_in_dim(running, offset, offset + length, axis=0))
    return results


def chain(earlier, later):
    return (earlier[0] * later[0], later[0][:, :, None] * earlier[1] + later[1])


def to_blocks(tensor, block_count, head_count):
    return tensor.reshape(block_count, SPAN, head_count, RDIM).transpose(0, 2, 1, 3)


def local(
    tokens,
    norm_gain,
    pool_in_weight,
    query_weight,
    forget_weight,
    input_weight,
    forget_gap,
    decay_shift,
    out_gain,
    pool_out_weight,
    recur_out_weight,
):
    pool_cols = pool_in_weight.shape[1]
    recur_cols = query_weight.shape[1]
    local_in = jnp.concatenate([pool_in_weight, query_weight, forget_weight, input_weight], axis=1)
    whole_in = lax.all_gather(local_in, "sp", axis=0, tiled=True)
    floats = tokens.astype(jnp.float32)
    scale = lax.rsqrt(jnp.mean(floats * floats, axis=-1, keepdims=True) + EPSILON)
    normed = (floats * scale * norm_gain).astype(jnp.bfloat16)
    pool_weight = whole_in[:, :pool_cols]
    recur_weight = whole_in[:, pool_cols:]
    pooled_in = jnp.dot(
        lax.all_gather(normed, "tp", axis=0, tiled=True),
        pool_weight,
        preferred_element_type=jnp.float32,
    ).astype(jnp.bfloat16)
    recur_in = jnp.dot(
        lax.all_gather(normed, "tp", axis=0, tiled=True),
        recur_weight,
        preferred_element_type=jnp.float32,
    ).astype(jnp.bfloat16)
    query = recur_in[:, :recur_cols].astype(jnp.float32)
    forget_pre = recur_in[:, recur_cols : 2 * recur_cols].astype(jnp.float32)
    values = recur_in[:, 2 * recur_cols :].astype(jnp.float32)
    row_count = pooled_in.shape[0]
    head_count = recur_cols // RDIM
    block_count = row_count // SPAN
    gate_pre = forget_pre.reshape(row_count, head_count, RDIM)
    opened = forget_gap.reshape(head_count, RDIM) * jax.nn.sigmoid(-gate_pre)
    log_decay = jnp.log1p(-opened) + decay_shift.T[:, :, None]
    query_blocks = to_blocks(query, block_count, head_count)
    decay_blocks = to_blocks(log_decay, block_count, head_count)
    key_blocks = to_blocks(opened, block_count, head_count)
    value_blocks = to_blocks(values, block_count, head_count)
    causal = jnp.tril(jnp.ones((SPAN, SPAN), jnp.bool_))
    inner_block_output = jnp.cumsum(decay_blocks, axis=2)
    block_decay_total = inner_block_output[:, :, -1, :]
    decayed_query = query_blocks * jnp.exp(inner_block_output)
    scores = jnp.einsum(
        "bhtk,bhsk->bhts",
        decayed_query,
        key_blocks * jnp.exp(-inner_block_output),
        precision=EXACT_MATMUL,
    )
    scores = jnp.where(causal, scores, 0.0)
    received_output = jnp.einsum("bhts,bhsv->bhtv", scores, value_blocks, precision=EXACT_MATMUL)
    growth_factor = jnp.einsum(
        "bhsk,bhsv->bhkv",
        key_blocks * jnp.exp(block_decay_total[:, :, None, :] - inner_block_output),
        value_blocks,
        precision=EXACT_MATMUL,
    )
    fading = jnp.exp(block_decay_total)

    def carry_step(state_matrix, item):
        return (item[0][:, :, None] * state_matrix + item[1], state_matrix)

    empty_state = jnp.zeros((head_count, RDIM, RDIM), jnp.float32)
    local_state, block_starts = lax.scan(carry_step, empty_state, (fading, growth_factor))
    received_output = received_output + jnp.einsum(
        "bhtk,bhkv->bhtv", decayed_query, block_starts, precision=EXACT_MATMUL
    )
    earlier_total = jnp.cumsum(block_decay_total, axis=0) - block_decay_total
    decay_from_start = query_blocks * jnp.exp(inner_block_output + earlier_total[:, :, None, :])
    device_fade = jnp.exp(jnp.sum(block_decay_total, axis=0))
    reach = 2**GROUPS - 1
    rim = pooled_in[row_count - reach :]
    unit_fade = jnp.ones((head_count, RDIM), jnp.float32)
    previous = passed_along(rim, "sp", 1)
    carried_fade, carried_state = prefix(
        (device_fade, local_state), "sp", chain, (unit_fade, empty_state)
    )
    received_output = received_output + jnp.einsum(
        "fuoy,uyi->fuoi", decay_from_start, carried_state, precision=EXACT_MATMUL
    )
    received_output = received_output.transpose(0, 2, 1, 3).reshape(row_count, head_count, RDIM)
    spread = lax.rsqrt(
        jnp.mean(received_output * received_output, axis=-1, keepdims=True) + EPSILON
    )
    recur_mixed = (
        (received_output * spread * out_gain).astype(jnp.bfloat16).reshape(row_count, recur_cols)
    )
    group = lax.axis_index("tp")
    padded = jnp.concatenate([previous, pooled_in], axis=0).astype(jnp.float32)
    results = window_sums(padded, GROUPS, reach)
    window_sum = results[GROUPS - 1]
    for level in range(GROUPS - 1):
        window_sum = jnp.where(group == level, results[level], window_sum)
    width = jnp.left_shift(jnp.int32(2), group)
    position = lax.axis_index("sp") * row_count + jnp.arange(row_count, dtype=jnp.int32)
    divisor = jnp.minimum(position + 1, width).astype(jnp.float32)[:, None]
    pool_mixed = (window_sum / divisor - pooled_in.astype(jnp.float32)).astype(jnp.bfloat16)
    out_pool, out_recur = (
        lax.all_gather(pool_out_weight, "sp", axis=1, tiled=True),
        lax.all_gather(recur_out_weight, "sp", axis=1, tiled=True),
    )
    partial_value = jnp.dot(pool_mixed, out_pool, preferred_element_type=jnp.float32)
    return lax.psum_scatter(
        (
            partial_value + jnp.dot(recur_mixed, out_recur, preferred_element_type=jnp.float32)
        ).astype(jnp.bfloat16),
        "tp",
        scatter_dimension=0,
        tiled=True,
    )


RING = 4
CHUNK = 128
MESH = pl.DeviceIdType.MESH
NT = (((1,), (1,)), ((), ()))
TN = (((0,), (0,)), ((), ()))


def matmul(a, b, dims=(((1,), (0,)), ((), ()))):
    return lax.dot_general(a, b, dims, preferred_element_type=jnp.float32)


class Relay:
    def __init__(self, slots, send, recv, place):
        z, self.x = place // 2, place % 2
        self.slots, self.send, self.recv = slots, send, recv
        self.place, self.began = place, []
        self.partner = place + 1 - 2 * self.x
        mate, half = z + 1 - 2 * (z % 2), z // 2
        self.mate = 2 * mate + self.x
        self.across = 2 * lax.rem(RING + RING - 1 - z, RING) + self.x
        self.middle = (z + half) % 2 == 1
        self.end = (z + half) % 2 == 0
        self.line = [mate, 2 - half, 3 - 3 * half]

    def copy(self, k, owner, target, half=None):
        block = self.slots.at[owner]
        if half is not None:
            size = self.slots.shape[1] // 2
            block = self.slots.at[owner, pl.ds(half * size, size)]
        return pltpu.make_async_remote_copy(
            src_ref=block,
            dst_ref=block,
            send_sem=self.send.at[k],
            recv_sem=self.recv.at[owner],
            device_id={"sp": target},
            device_id_type=MESH,
        )

    def start(self, k, owner, target, gate=None, half=None):
        copy = self.copy(k, owner, target, half)
        self.began.append((copy, gate))
        if gate is None:
            copy.start()
        else:
            pl.when(gate)(copy.start)

    def arrived(self, owner):
        self.copy(0, owner, self.partner).wait_recv()

    def column(self, k):
        return 2 * self.line[k] + self.x

    def across_x(self, k):
        return 2 * self.line[k] + 1 - self.x

    def open(self):
        self.start(0, self.place, self.partner)
        self.start(1, self.place, self.mate)
        self.start(2, self.place, self.across, self.middle)

    def hop(self, k):
        owner = self.column(k)
        self.arrived(owner)
        target = self.mate if k else self.across
        self.start(3 + 2 * k, owner, target, self.middle)
        over_x = (self.middle, self.end, None)[k]
        self.start(4 + 2 * k, owner, self.partner, over_x)
        if k == 0:
            self.start(11, owner, self.partner, self.end, 0)

    def inward(self):
        self.arrived(self.partner)
        self.start(9, self.partner, self.across, self.middle)
        self.start(10, self.partner, self.mate, self.middle, 1)

    def close(self):
        for copy, gate in self.began:
            if gate is None:
                copy.wait_send()
            else:
                pl.when(gate)(copy.wait_send)


def fused_kernel(
    blocks,
    parts,
    tokens_ref,
    gain_ref,
    pool_in_ref,
    query_ref,
    forget_ref,
    input_ref,
    gap_ref,
    shift_ref,
    out_gain_ref,
    pool_out_ref,
    recur_out_ref,
    out_ref,
    normed,
    win,
    wout,
    acc,
    pooled,
    rim,
    state_out,
    state_near,
    state_pair,
    state_in,
    fade_out,
    fade_near,
    fade_pair,
    fade_in,
    dq_ref,
    heard_ref,
    mixed,
    part,
    part_in,
    pair,
    in_send,
    in_recv,
    out_send,
    out_recv,
    tok_send,
    tok_recv,
    rim_sem,
    state_send,
    state_recv,
    fade_send,
    fade_recv,
    part_send,
    part_recv,
    local_sem,
):
    place, seat = lax.axis_index("sp"), lax.axis_index("tp")
    partner = place + 1 - 2 * (place % 2)
    rows, width = tokens_ref.shape
    depth, cols = pool_in_ref.shape
    z, x = place // 2, place % 2
    length = rows * parts
    heads = cols // RDIM

    staged_in, staged_out = [], []
    for i, ref in enumerate((pool_in_ref, query_ref, forget_ref, input_ref)):
        target = win.at[place, :, pl.ds(i * cols, cols)]
        staged_in.append(pltpu.make_async_copy(ref, target, local_sem.at[i]))
        staged_in[-1].start()
    for i, ref in enumerate((pool_out_ref, recur_out_ref)):
        target = wout.at[place, pl.ds(i * cols, cols)]
        staged_out.append(pltpu.make_async_copy(ref, target, local_sem.at[4 + i]))
        staged_out[-1].start()
    barrier = pltpu.get_barrier_semaphore()
    for d in range(1, blocks):
        peer = lax.rem(place + d, blocks)
        pl.semaphore_signal(barrier, inc=1, device_id={"sp": peer}, device_id_type=MESH)
    for d in range(1, parts):
        peer = lax.rem(seat + d, parts)
        pl.semaphore_signal(barrier, inc=1, device_id={"tp": peer}, device_id_type=MESH)
    floats = tokens_ref[...].astype(jnp.float32)
    scale = lax.rsqrt(jnp.mean(floats * floats, axis=-1, keepdims=True) + EPSILON)
    normed[seat] = (floats * scale * gain_ref[...]).astype(jnp.bfloat16)
    pl.semaphore_wait(barrier, blocks + parts - 2)

    for copy in staged_in:
        copy.wait()
    wins = Relay(win, in_send, in_recv, place)
    wouts = Relay(wout, out_send, out_recv, place)
    wins.open()
    toks = []
    for d in range(1, parts):
        toks.append(
            pltpu.make_async_remote_copy(
                src_ref=normed.at[seat],
                dst_ref=normed.at[seat],
                send_sem=tok_send.at[d - 1],
                recv_sem=tok_recv.at[d - 1],
                device_id={"tp": lax.rem(seat + d, parts)},
                device_id_type=MESH,
            )
        )
        toks[-1].start()

    def accumulate(block, owner, first=False):
        columns = pl.ds(pl.multiple_of(owner * depth, depth), depth)
        left = normed[:, :, columns].reshape(length, depth)

        @pl.loop(0, 4)
        def _(tile):
            at = pl.ds(pl.multiple_of(tile * cols, cols), cols)
            product = matmul(left, block[:, at])
            if first:
                acc[:, at] = product
            else:
                acc[:, at] += product

    wins.hop(0)
    wins.inward()
    wins.hop(1)
    for copy in toks:
        copy.wait_recv()
    accumulate(win.at[place], place, True)
    wins.hop(2)
    for copy in staged_out:
        copy.wait()
    wouts.open()
    for k in range(3):
        accumulate(win.at[wins.column(k)], wins.column(k))
    accumulate(win.at[partner], partner)
    for k in range(3):
        owner = wins.across_x(k)
        wins.arrived(owner)
        accumulate(win.at[owner], owner)

    pooled[...] = acc[:, :cols].astype(jnp.bfloat16)
    rim_rows = rim.shape[0]
    rims = pltpu.make_async_remote_copy(
        src_ref=pooled.at[pl.ds(length - rim_rows, rim_rows)],
        dst_ref=rim,
        send_sem=rim_sem.at[0],
        recv_sem=rim_sem.at[1],
        device_id={"sp": lax.rem(place + 1, blocks)},
        device_id_type=MESH,
    )
    rims.start()
    wouts.hop(0)
    wouts.inward()

    row = lax.broadcasted_iota(jnp.int32, (CHUNK, CHUNK), 0)
    col = lax.broadcasted_iota(jnp.int32, (CHUNK, CHUNK), 1)
    causal = col <= row
    lower = causal.astype(jnp.float32)
    for h in range(heads):
        lanes = slice(h * RDIM, (h + 1) * RDIM)
        state = jnp.zeros((RDIM, RDIM), jnp.float32)
        total = jnp.zeros((1, RDIM), jnp.float32)
        for b in range(length // CHUNK):
            at = slice(b * CHUNK, (b + 1) * CHUNK)

            def taken(kind):
                low = kind * cols + h * RDIM
                return acc[at, low : low + RDIM].astype(jnp.bfloat16)

            query = taken(1).astype(jnp.float32)
            gate = taken(2).astype(jnp.float32)
            values = taken(3)
            opened = gap_ref[:, lanes] * jax.nn.sigmoid(-gate)
            decay = jnp.log1p(-opened) + jnp.broadcast_to(shift_ref[h : h + 1, at], (RDIM, CHUNK)).T
            inner = lax.dot_general(
                lower,
                decay,
                (((1,), (0,)), ((), ())),
                precision=EXACT_MATMUL,
                preferred_element_type=jnp.float32,
            )
            last = inner[CHUNK - 1 :, :]
            asked = query * jnp.exp(inner)
            keys = (opened * jnp.exp(-inner)).astype(jnp.bfloat16)
            kept = (opened * jnp.exp(last - inner)).astype(jnp.bfloat16)
            asked16 = asked.astype(jnp.bfloat16)
            scores = jnp.where(causal, matmul(asked16, keys, NT), 0.0)
            heard = matmul(scores.astype(jnp.bfloat16), values)
            if b:
                heard += matmul(asked16, state.astype(jnp.bfloat16), NT)
            heard_ref[at, lanes] = heard
            dq_ref[at, lanes] = (asked * jnp.exp(total)).astype(jnp.bfloat16)
            state = jnp.exp(last) * state + matmul(values, kept, TN)
            total = total + last
        state_out[h] = state.astype(jnp.bfloat16)
        fade_out[h] = jnp.broadcast_to(jnp.exp(total), (8, RDIM))

    kinds = (
        (fade_out, fade_near, fade_pair, fade_in, fade_send, fade_recv),
        (state_out, state_near, state_pair, state_in, state_send, state_recv),
    )
    states, later = [], []
    for own, near_ref, _, _, send, recv in kinds:
        copy = pltpu.make_async_remote_copy(
            src_ref=own,
            dst_ref=near_ref,
            send_sem=send.at[0],
            recv_sem=recv.at[0],
            device_id={"sp": partner},
            device_id_type=MESH,
        )
        copy.start()
        states.append(copy)
    wouts.hop(1)
    for copy in states:
        copy.wait_recv()
    for h in range(heads):
        fades = fade_out[h], fade_near[h]
        ours, theirs = state_out[h].astype(jnp.float32), state_near[h].astype(jnp.float32)
        first = jnp.where(x == 0, ours, theirs)
        second = jnp.where(x == 0, theirs, ours)
        fade_pair[h] = fades[0] * fades[1]
        fade = jnp.where(x == 0, fades[1], fades[0])[:1]
        state_pair[h] = (fade * first + second).astype(jnp.bfloat16)
    for d in range(1, RING):
        for _, _, pair_ref, dst, send, recv in kinds:
            copy = pltpu.make_async_remote_copy(
                src_ref=pair_ref,
                dst_ref=dst.at[z],
                send_sem=send.at[d],
                recv_sem=recv.at[d],
                device_id={"sp": lax.rem(place + 2 * d, blocks)},
                device_id_type=MESH,
            )
            pl.when(z + d < RING)(copy.start)
            later.append((d, copy))
    wouts.hop(2)

    rims.wait_recv()
    before = jnp.where(place > 0, rim[...].astype(jnp.float32), 0.0)
    here = pooled[...].astype(jnp.float32)
    running = jnp.concatenate([before, here], axis=0)
    chosen = None
    for level in range(GROUPS):
        running = running + pltpu.roll(running, 2**level, axis=0)
        chosen = running if level == 0 else jnp.where(seat >= level, running, chosen)
    window = jnp.left_shift(jnp.int32(2), seat)
    position = place * length + lax.broadcasted_iota(jnp.int32, (length, 1), 0)
    divisor = jnp.minimum(position + 1, window).astype(jnp.float32)
    mixed[:, :cols] = (chosen[rim_rows:] / divisor - here).astype(jnp.bfloat16)

    for d, copy in later:
        pl.when(z >= d)(copy.wait_recv)
    for h in range(heads):
        lanes = slice(h * RDIM, (h + 1) * RDIM)
        carried = jnp.zeros((RDIM, RDIM), jnp.float32)
        for j in range(RING - 1):
            grown = fade_in[j, h][:1] * carried + state_in[j, h].astype(jnp.float32)
            carried = jnp.where(j < z, grown, carried)
        grown = fade_near[h][:1] * carried + state_near[h].astype(jnp.float32)
        carried = jnp.where(x == 1, grown, carried)
        heard = heard_ref[:, lanes] + matmul(dq_ref[:, lanes], carried.astype(jnp.bfloat16), NT)
        spread = lax.rsqrt(jnp.mean(heard * heard, axis=-1, keepdims=True) + EPSILON)
        low = cols + h * RDIM
        mixed[:, low : low + RDIM] = (heard * spread * out_gain_ref[...]).astype(jnp.bfloat16)

    step = wout.shape[2]
    left = mixed[...]
    other = 2 * (1 - seat // 2) + seat % 2
    near = seat + 1 - 2 * (seat % 2)
    cross = other + 1 - 2 * (seat % 2)
    sums, chunks = [], []

    def send_part(src, lane, target, at):
        copy = pltpu.make_async_remote_copy(
            src_ref=src,
            dst_ref=part_in.at[lane, :, at],
            send_sem=part_send.at[len(sums)],
            recv_sem=part_recv.at[len(sums)],
            device_id={"tp": target},
            device_id_type=MESH,
        )
        copy.start()
        sums.append(copy)
        return copy

    def pass_on(chunk):
        at, relayed = chunk[0], chunk[1]
        relayed.wait_recv()
        both = part[other, :, at].astype(jnp.float32) + part_in[0, :, at].astype(jnp.float32)
        pair[:, at] = both.astype(jnp.bfloat16)
        chunk.append(send_part(pair.at[:, at], 2, other, at))

    for j in range(RING):
        if j:
            wouts.arrived(wouts.across_x(j - 1))
        base = 2 * (wouts.line[j - 1] if j else z)
        for i in (base, base + 1):
            at = pl.ds(pl.multiple_of(i * step, step), step)
            part[:, :, at] = matmul(left, wout[i]).astype(jnp.bfloat16).reshape(parts, rows, step)
        at = pl.ds(pl.multiple_of(base * step, 2 * step), 2 * step)
        relayed = send_part(part.at[cross, :, at], 0, near, at)
        chunks.append([at, relayed, send_part(part.at[near, :, at], 1, near, at)])
        if j:
            pass_on(chunks[-2])
    pass_on(chunks[-1])
    for at, _, nearby, far in chunks:
        nearby.wait_recv()
        total = part[seat, :, at].astype(jnp.float32) + part_in[1, :, at].astype(jnp.float32)
        far.wait_recv()
        out_ref[:, at] = (total + part_in[2, :, at].astype(jnp.float32)).astype(jnp.bfloat16)
    wins.close()
    wouts.close()
    for copy in toks + [rims] + states + sums:
        copy.wait_send()
    for d, copy in later:
        pl.when(z + d < RING)(copy.wait_send)


def fused(
    blocks,
    parts,
    tokens,
    norm_gain,
    pool_in_weight,
    query_weight,
    forget_weight,
    input_weight,
    forget_gap,
    decay_shift,
    out_gain,
    pool_out_weight,
    recur_out_weight,
):
    rows, width = tokens.shape
    length = rows * parts
    depth, cols = pool_in_weight.shape
    heads = cols // RDIM
    step = pool_out_weight.shape[1]
    bf16, f32 = jnp.bfloat16, jnp.float32
    seats = parts - 1
    vmem, whole = pl.BlockSpec(memory_space=pltpu.VMEM), pl.BlockSpec(memory_space=pl.ANY)
    sem = pltpu.SemaphoreType.DMA
    return pl.pallas_call(
        functools.partial(fused_kernel, blocks, parts),
        out_shape=jax.ShapeDtypeStruct((rows, width), bf16),
        in_specs=[vmem] * 2 + [whole] * 4 + [vmem] * 3 + [whole] * 2,
        out_specs=pl.BlockSpec(memory_space=pltpu.VMEM),
        scratch_shapes=[
            pltpu.VMEM((parts, rows, width), bf16),
            pltpu.VMEM((blocks, depth, 4 * cols), bf16),
            pltpu.VMEM((blocks, 2 * cols, step), bf16),
            pltpu.VMEM((length, 4 * cols), f32),
            pltpu.VMEM((length, cols), bf16),
            pltpu.VMEM((2**GROUPS, cols), bf16),
            *[pltpu.VMEM((heads, RDIM, RDIM), bf16)] * 3,
            pltpu.VMEM((RING, heads, RDIM, RDIM), bf16),
            *[pltpu.VMEM((heads, 8, RDIM), f32)] * 3,
            pltpu.VMEM((RING, heads, 8, RDIM), f32),
            pltpu.VMEM((length, cols), bf16),
            pltpu.VMEM((length, cols), f32),
            pltpu.VMEM((length, 2 * cols), bf16),
            pltpu.VMEM((parts, rows, width), bf16),
            pltpu.VMEM((seats, rows, width), bf16),
            pltpu.VMEM((rows, width), bf16),
            sem((12,)),
            sem((blocks,)),
            sem((12,)),
            sem((blocks,)),
            sem((seats,)),
            sem((seats,)),
            sem((2,)),
            sem((RING,)),
            sem((RING,)),
            sem((RING,)),
            sem((RING,)),
            sem((seats * blocks // 2,)),
            sem((seats * blocks // 2,)),
            sem((6,)),
        ],
        compiler_params=pltpu.CompilerParams(
            collective_id=0, has_side_effects=True, vmem_limit_bytes=60000 * 1024
        ),
    )(
        tokens,
        norm_gain.reshape(1, width),
        pool_in_weight,
        query_weight,
        forget_weight,
        input_weight,
        forget_gap.reshape(1, cols),
        decay_shift,
        out_gain.reshape(1, RDIM),
        pool_out_weight,
        recur_out_weight,
    )


def solution(mesh):
    blocks, parts = mesh.shape["sp"], mesh.shape["tp"]
    body = functools.partial(fused, blocks, parts) if (blocks, parts) == (2 * RING, RING) else local
    in_specs = (
        P(("sp", "tp"), None),
        P(),
        P("sp", "tp"),
        P("sp", "tp"),
        P("sp", "tp"),
        P("sp", "tp"),
        P("tp"),
        P("tp", "sp"),
        P(),
        P("tp", "sp"),
        P("tp", "sp"),
    )
    out_specs = P(("sp", "tp"), None)
    return jax.shard_map(body, mesh=mesh, in_specs=in_specs, out_specs=out_specs, check_vma=False)
```
